32 devices in a mesh: fs: 16 (over z, y, x), tp: 2 (over core).
Axes of the slice: x: 2, y: 2, z: 4, core: 2. Of those that a mesh axis runs over, the one named last changes fastest.
Arguments:
- x_late: bfloat16 [4096, 2048], P('fs'), may hold values from -6 to 6
- x_early: bfloat16 [4096, 2048], P('fs'), may hold values from -6 to 6
- cotangent: bfloat16 [4096, 2048], P('fs'), may hold values from -6 to 6
- w_gate: bfloat16 [2048, 4096], P('fs', 'tp'), may hold values from -0.125 to 0.125
- w_up: bfloat16 [2048, 4096], P('fs', 'tp'), may hold values from -0.125 to 0.125
- w_down: bfloat16 [4096, 2048], P('tp', 'fs'), may hold values from -0.09375 to 0.09375
- conv_taps: float32 [3, 4096], replicated, may hold values from -3 to 3
- conv_bias: float32 [4096], replicated, may hold values from -3 to 3
- grad_down: float32 [4096, 2048], P('tp', 'fs'), may hold values from -60 to 60
Outputs:
- y_late: bfloat16 [4096, 2048], P('fs')
- dx_early: bfloat16 [4096, 2048], P('fs')
- grad_down_out: float32 [4096, 2048], P('tp', 'fs')
The draws below stay inside these ranges and needn't reach their ends.
All inputs are finite; a program needn't handle non-finite values.
Results may differ from the reference program's by a relative error of at most 0.017.
Values may be sent and summed in bfloat16 or wider, within the bound.
A program may use at most 128 MiB of HBM per device.

```python
import jax
import jax.numpy as jnp
from jax import lax

D = 2048
FF = 4096
TAPS = 3
TOK_DEV = 256
TOKENS = 4096
N_FS = 16
N_TP = 2


def strengthened(array, stream_key, source, target, blocks, factor):
    owner, partner = [(jnp.arange(array.shape[dim]) // (array.shape[dim] // blocks)).reshape([-1 if axis == dim else 1 for axis in range(array.ndim)]) for dim in (source, target)]
    chosen = jax.random.permutation(stream_key, blocks)[partner]
    strong = (owner == chosen) | (owner == (partner + blocks // 2) % blocks)
    return jnp.where(strong, factor * array, array)


def shard_levels(rng, dims, shards, smallest, top_value):
    level, own = 1.0, jax.random.fold_in(rng, 6)
    for axis_at, parts in shards:
        steps = jnp.exp(jax.random.uniform(jax.random.fold_in(own, axis_at), (parts,), jnp.float32, smallest / len(shards), top_value / len(shards)))
        level = level * jnp.repeat(steps, dims[axis_at] // parts).reshape([-1 if axis == axis_at else 1 for axis in range(len(dims))])
    return level


def scatter_about(rng, dims, spread, bound, cuts=(), dtype=jnp.bfloat16):
    loudness = shard_levels(rng, dims, cuts, -0.22, 0.18) if cuts else 1.0
    array = jax.random.normal(rng, dims, jnp.float32) * spread * loudness
    return jnp.minimum(jnp.maximum(array, -bound), bound).astype(dtype)


def bell_draw_with(key, dims, scale, bound, split, heavy, held_as=jnp.bfloat16):
    values = scale * jax.random.normal(key, dims, jnp.float32)
    if split:
        values = values * shard_levels(key, dims, split, -0.22, 0.18)
    return jnp.clip(strengthened(values, jax.random.fold_in(key, 3), *heavy), -bound, bound).astype(held_as)


def setup_inputs(seed: int = 0) -> dict:
    streams_of = jax.random.split(jax.random.key(seed), 10)
    x_late = scatter_about(streams_of[0], (TOKENS, D), 1.0, 6.0, ((0, 16),))
    x_early = scatter_about(streams_of[1], (TOKENS, D), 1.0, 6.0, ((0, 16),))
    cotangent = bell_draw_with(streams_of[2], (TOKENS, D), 1.0, 6.0, ((0, 16),), (0, 1, 16, 2.0))
    w_gate = scatter_about(streams_of[3], (D, FF), D ** -0.5, 0.125, ((0, 16), (1, 2)))
    w_up = scatter_about(streams_of[4], (D, FF), D ** -0.5, 0.125, ((0, 16), (1, 2)))
    w_down = scatter_about(streams_of[5], (FF, D), FF ** -0.5, 0.09375, ((0, 2), (1, 16)))
    conv_taps = scatter_about(streams_of[6], (TAPS, FF), 0.6, 3.0, (), jnp.float32)
    conv_bias = scatter_about(streams_of[7], (FF,), 0.5, 3.0, (), jnp.float32)
    grad_down = scatter_about(streams_of[8], (FF, D), 10.0, 60.0, ((0, 2), (1, 16)), jnp.float32)
    return {"x_late": x_late, "x_early": x_early, "cotangent": cotangent, "w_gate": w_gate, "w_up": w_up, "w_down": w_down, "conv_taps": conv_taps, "conv_bias": conv_bias, "grad_down": grad_down}


def shift_later(field, steps):
    pad = jnp.zeros((field.shape[0], steps, field.shape[2]), jnp.float32)
    return jnp.concatenate([pad, field[:, :field.shape[1] - steps]], axis=1)


def shift_earlier(field, steps):
    pad = jnp.zeros((field.shape[0], steps, field.shape[2]), jnp.float32)
    return jnp.concatenate([field[:, steps:], pad], axis=1)


def mlp_parts(inputs, w_gate, w_up, conv_taps, conv_bias):
    gate = jnp.dot(inputs, w_gate, preferred_element_type=jnp.float32).astype(jnp.bfloat16)
    up = jnp.dot(inputs, w_up, preferred_element_type=jnp.float32)
    seqs = gate.astype(jnp.float32).reshape(N_FS, TOK_DEV, FF)
    conv = conv_bias + conv_taps[2] * seqs + conv_taps[1] * shift_later(seqs, 1) + conv_taps[0] * shift_later(seqs, 2)
    conv = conv.reshape(TOKENS, FF)
    act = jax.nn.silu(conv)
    hidden = (act * up).astype(jnp.bfloat16)
    return conv, act, up, hidden


def rounded(value):
    return lax.optimization_barrier(value.astype(jnp.bfloat16)).astype(jnp.float32)


def reference(x_late, x_early, cotangent, w_gate, w_up, w_down, conv_taps, conv_bias, grad_down):
    width = FF // N_TP
    conv, act, up, hidden = mlp_parts(x_late, w_gate, w_up, conv_taps, conv_bias)
    total = jnp.zeros((TOKENS, D), jnp.float32)
    for block in range(N_TP):
        lo = block * width
        total = total + rounded(jnp.dot(hidden[:, lo:lo + width], w_down[lo:lo + width], preferred_element_type=jnp.float32))
    y_late = total.astype(jnp.bfloat16)

    conv, act, up, hidden = mlp_parts(x_early, w_gate, w_up, conv_taps, conv_bias)
    dhidden = jnp.dot(cotangent, w_down.T, preferred_element_type=jnp.float32)
    dup = (dhidden * act).astype(jnp.bfloat16)
    sig = jax.nn.sigmoid(conv)
    dconv = (dhidden * up * sig * (1.0 + conv * (1.0 - sig))).reshape(N_FS, TOK_DEV, FF)
    dgate = conv_taps[2] * dconv + conv_taps[1] * shift_earlier(dconv, 1) + conv_taps[0] * shift_earlier(dconv, 2)
    dgate = dgate.reshape(TOKENS, FF).astype(jnp.bfloat16)
    total = jnp.zeros((TOKENS, D), jnp.float32)
    for block in range(N_TP):
        lo = block * width
        part = jnp.dot(dup[:, lo:lo + width], w_up[:, lo:lo + width].T, preferred_element_type=jnp.float32)
        part = part + jnp.dot(dgate[:, lo:lo + width], w_gate[:, lo:lo + width].T, preferred_element_type=jnp.float32)
        total = total + rounded(part)
    dx_early = total.astype(jnp.bfloat16)
    grad_down_out = grad_down + jnp.dot(hidden.T, cotangent, preferred_element_type=jnp.float32)
    return y_late, dx_early, grad_down_out
```

```python
import functools

import jax
import jax.numpy as jnp
from jax import lax
from jax.experimental import pallas as pl
from jax.experimental.pallas import tpu as pltpu
from jax.sharding import PartitionSpec as P

GROUP = 4
VMEM_BYTES = 63 * 1024 * 1024
VMEM = pl.BlockSpec(memory_space=pltpu.VMEM)


def place():
    f, c = lax.axis_index("fs"), lax.axis_index("tp")
    q, z = lax.rem(f, GROUP), lax.div(f, GROUP)
    qx = q + 1 - 2 * lax.rem(q, 2)
    qy = q + 2 - 4 * lax.div(q, 2)
    qa, qb = qx + c * (qy - qx), qy + c * (qx - qy)
    return f, c, q, z, qa, qb, GROUP - 1 - q


def at(start, size):
    return pl.ds(pl.multiple_of(start, size), size)


def remote(src, dst, send, recv, **device):
    return pltpu.make_async_remote_copy(
        src_ref=src, dst_ref=dst, send_sem=send, recv_sem=recv,
        device_id=device, device_id_type=pl.DeviceIdType.MESH,
    )


def total(dst, srcs, rows, step=32):
    @pl.loop(0, rows, step=step)
    def _(i):
        sl = pl.ds(pl.multiple_of(i, step), step)
        out = srcs[0][sl, :].astype(jnp.float32)
        for s in srcs[1:]:
            out = out + s[sl, :].astype(jnp.float32)
        dst[sl, :] = out.astype(dst.dtype)


def mm(left, right, dims=((1,), (0,))):
    return lax.dot_general(left, right, (dims, ((), ())), preferred_element_type=jnp.float32)


def layer_kernel(nz, tile, x0, x1, x2, wg, wu, wd, taps, bias, gd, y, dx, g,
                 t0, t1, t2, og, ou, od, hid, hid_t, conv_s, up_s, dup, dgate, yp, xp, gp,
                 core, summed, got, gin_r, gin_l, gsum, hand,
                 loc, w_s, w_r, n_s, n_r, p_s, p_r, r_s, r_r, l_s, l_r,
                 c_s, c_r, a_s, a_r, zr_s, zr_r, zl_s, zl_r, g_s, g_r, e_s, e_r):
    f, c, q, z, qa, qb, qd = place()
    base = z * GROUP
    xs, ts, outs = (x0, x1, x2), (t0, t1, t2), (og, ou, od)
    rows, d_model = x0.shape
    half = rows // 2
    r, u = wg.shape[0], og.shape[1]
    wide = GROUP * r
    first, last = z > 0, z < nz - 1
    low, high = z == 0, z == nz - 1
    units = (c * GROUP + q) * u

    barrier = pltpu.get_barrier_semaphore()
    for peer in (qa, qb, qd):
        pl.semaphore_signal(barrier, 1, device_id={"fs": base + peer}, device_id_type=pl.DeviceIdType.MESH)
    pl.semaphore_signal(barrier, 1, device_id={"tp": 1 - c}, device_id_type=pl.DeviceIdType.MESH)
    for s in range(1, nz):
        pl.semaphore_signal(barrier, 1, device_id={"fs": lax.rem(z + s, nz) * GROUP + q},
                            device_id_type=pl.DeviceIdType.MESH)
    pl.semaphore_wait(barrier, 3 + nz)

    def piece(k, peer):
        if k == 2:
            return wd.at[at(peer * u, u), :]
        return (wg, wu)[k].at[:, at(peer * u, u)]

    def landing(k, owner):
        if k == 2:
            return od.at[:, at(owner * r, r)]
        return outs[k].at[at(owner * r, r), :]

    def block(k, b):
        if k == 2:
            return od.at[:, at(b * wide, wide)]
        return outs[k].at[at(b * wide, wide), :]

    def right(k, s):
        b = block(k, z - s)
        return remote(b, b, r_s.at[s, k], r_r.at[s, k], fs=f + GROUP)

    def left(k, s):
        b = block(k, z + s)
        return remote(b, b, l_s.at[s, k], l_r.at[s, k], fs=f - GROUP)

    def from_left(k, s):
        b = block(k, z - s - 1)
        return remote(b, b, r_s.at[s, k], r_r.at[s, k], fs=f - GROUP)

    def from_right(k, s):
        b = block(k, z + s + 1)
        return remote(b, b, l_s.at[s, k], l_r.at[s, k], fs=f + GROUP)

    def onward(k, s, act):
        @pl.when(jnp.logical_and(z - s >= 0, last))
        def _():
            act(right(k, s))

        @pl.when(jnp.logical_and(z + s < nz, first))
        def _():
            act(left(k, s))

    begin, sent = (lambda copy: copy.start()), (lambda copy: copy.wait_send())

    def along(k, src, owner):
        there = landing(k, owner)

        @pl.when(last)
        def _():
            remote(src, there, r_s.at[0, k], r_r.at[0, k], fs=f + GROUP).start()

        @pl.when(first)
        def _():
            remote(src, there, l_s.at[0, k], l_r.at[0, k], fs=f - GROUP).start()

    def relay(k, s):
        @pl.when(jnp.logical_and(z - s - 1 >= 0, last))
        def _():
            from_left(k, s).wait_recv()
            right(k, s + 1).start()

        @pl.when(jnp.logical_and(z + s + 1 < nz, first))
        def _():
            from_right(k, s).wait_recv()
            left(k, s + 1).start()

    def ended(k, s):
        @pl.when(high)
        def _():
            from_left(k, s).wait_recv()

        @pl.when(low)
        def _():
            from_right(k, s).wait_recv()

    mine, other = at(c * half, half), at((1 - c) * half, half)
    weights, near, local = {}, {}, []

    def spread(k):
        for d, peer in enumerate((qa, qb, qd)):
            copy = remote(piece(k, peer), landing(k, f), w_s.at[k, d], w_r.at[k, d], fs=base + peer)
            copy.start()
            weights[k, d] = copy

    def share(i):
        for d, peer in enumerate((qa, qb)):
            copy = remote(xs[i].at[mine, :], ts[i].at[q, mine, :], n_s.at[i, d], n_r.at[i, d], fs=base + peer)
            copy.start()
            near[i, d] = copy

    along(0, piece(0, q), f)
    spread(0)
    along(1, piece(1, q), f)
    spread(1)
    share(1)
    share(0)
    spread(2)
    share(2)
    for k in range(3):
        copy = pltpu.make_async_copy(piece(k, q), landing(k, f), loc.at[k])
        copy.start()
        local.append(copy)
    for i in range(3):
        copy = pltpu.make_async_copy(xs[i], ts[i].at[q], loc.at[3 + i])
        copy.start()
        local.append(copy)

    row = lax.broadcasted_iota(jnp.int32, (rows, tile), 0)

    def later(v, steps):
        return jnp.where(row >= steps, pltpu.roll(v, steps, 0), 0.0)

    def earlier(v, steps):
        return jnp.where(row < rows - steps, pltpu.roll(v, rows - steps, 0), 0.0)

    def forward(t, keep):
        @pl.loop(0, GROUP)
        def _(b):
            @pl.loop(0, u // tile)
            def _(j):
                cols, seq, par = at(j * tile, tile), at(b * rows, rows), at(units + j * tile, tile)
                x = t[b]
                gate = mm(x, og[:, cols]).astype(jnp.bfloat16).astype(jnp.float32)
                up = mm(x, ou[:, cols])
                conv = (bias[:, par] + taps[2:3, par] * gate + taps[1:2, par] * later(gate, 1)
                        + taps[0:1, par] * later(gate, 2))
                out = conv / (1.0 + jnp.exp(-conv)) * up
                if keep:
                    conv_s[seq, cols] = conv
                    up_s[seq, cols] = up
                    hid_t[at(j * tile, tile), seq] = out.T.astype(jnp.bfloat16)
                else:
                    hid[seq, cols] = out.astype(jnp.bfloat16)

    upper = lax.div(2 * z, nz)

    def down_grad():
        for i in range(nz):
            o = nz - 1 - i + upper * (2 * i - (nz - 1))
            cols = at(o * wide, wide)
            cot = t2[:, :, cols].reshape(GROUP * rows, wide)
            gp[:, cols] = mm(hid_t[...], cot).astype(jnp.bfloat16)
            if i < nz - 1:
                @pl.when(low)
                def _():
                    remote(gp.at[:, cols], gin_r.at[i], zr_s.at[i], zr_r.at[i], fs=f + GROUP).start()

                @pl.when(high)
                def _():
                    remote(gp.at[:, cols], gin_l.at[i], zl_s.at[i], zl_r.at[i], fs=f - GROUP).start()

    def gone(i):
        cols = at((nz - 1 - i) * wide, wide)
        return remote(gp.at[:, cols], gin_r.at[i], zr_s.at[i], zr_r.at[i], fs=f + GROUP)

    def chain(j):
        o = nz - 2 + z - j
        got_r = remote(gin_r.at[j], gin_r.at[j], zr_s.at[j], zr_r.at[j], fs=f - GROUP)
        got_l = remote(gin_l.at[j], gin_l.at[j], zl_s.at[j], zl_r.at[j], fs=f + GROUP)

        @pl.when(jnp.logical_and(first, o <= nz - 1))
        def _():
            got_r.wait_recv()

        if j < nz - 2:
            @pl.when(jnp.logical_and(first, o <= nz - 1))
            def _():
                cols = at(o * wide, wide)
                total(gp.at[:, cols], [gp.at[:, cols], gin_r.at[j]], u)
                remote(gp.at[:, cols], gin_r.at[j + 1], zr_s.at[j + 1], zr_r.at[j + 1], fs=f + GROUP).start()

        p = z + 1 - nz + 1 + j

        @pl.when(jnp.logical_and(last, p >= 0))
        def _():
            got_l.wait_recv()

        if j < nz - 2:
            @pl.when(jnp.logical_and(last, p >= 0))
            def _():
                cols = at(p * wide, wide)
                total(gp.at[:, cols], [gp.at[:, cols], gin_l.at[j]], u)
                remote(gp.at[:, cols], gin_l.at[j + 1], zl_s.at[j + 1], zl_r.at[j + 1], fs=f - GROUP).start()

    def backward():
        @pl.loop(0, GROUP)
        def _(b):
            @pl.loop(0, u // tile)
            def _(j):
                cols, seq, par = at(j * tile, tile), at(b * rows, rows), at(units + j * tile, tile)
                dh = mm(t2[b], od[at(j * tile, tile), :], ((1,), (1,)))
                conv = conv_s[seq, cols]
                sig = 1.0 / (1.0 + jnp.exp(-conv))
                dup[seq, cols] = (dh * (conv * sig)).astype(jnp.bfloat16)
                dc = dh * up_s[seq, cols] * sig * (1.0 + conv * (1.0 - sig))
                dg = (taps[2:3, par] * dc + taps[1:2, par] * earlier(dc, 1)
                      + taps[0:1, par] * earlier(dc, 2))
                dgate[seq, cols] = dg.astype(jnp.bfloat16)

    mirrored = z + upper * (nz - 1 - 2 * z)

    def turn(i):
        near_side = lax.div(mirrored - i + nz, nz)
        v = i + near_side * (mirrored - 2 * i)
        return v + upper * (nz - 1 - 2 * v)

    sub = 256 if wide % 256 == 0 else 128

    def late_block(i):
        start = turn(i) * wide

        @pl.loop(0, wide // sub)
        def _(j):
            cols = at(start + j * sub, sub)
            yp[:, cols] = mm(hid[...], od[:, cols]).astype(jnp.bfloat16)

    def early_block(i):
        @pl.loop(0, wide // sub)
        def _(j):
            cols = at(i * wide + j * sub, sub)
            part = mm(dup[...], ou[cols, :], ((1,), (1,))) + mm(dgate[...], og[cols, :], ((1,), (1,)))
            xp[:, cols] = part.astype(jnp.bfloat16)

    parts, finals = (yp, xp), (y, dx)
    order = (qd, qa, qb, q)
    theirs = (qd, qb, qa, q)
    cores, sends, ends = {}, {}, []

    def span(t, i):
        return at(turn(i) * wide, wide) if t == 0 else at(i * wide, wide)

    def to_core(t, i):
        cols = span(t, i)
        for n in range(4):
            src = parts[t].at[at(theirs[n] * rows + (1 - c) * half, half), cols]
            copy = remote(src, core.at[t, n, :, cols], c_s.at[t, i, n], c_r.at[t, i, n], tp=1 - c)
            copy.start()
            cores[t, i, n] = copy

    def send(t, i, src, slot, peer):
        cols = span(t, i)
        copy = remote(src, got.at[t, slot, :, cols], a_s.at[t, i, slot], a_r.at[t, i, slot], fs=base + peer)
        copy.start()
        sends[t, i, slot] = copy

    def join(t, i):
        cols = span(t, i)
        for n in range(4):
            cores[t, i, n].wait_recv()
            own = parts[t].at[at(order[n] * rows + c * half, half), cols]
            total(summed.at[t, n, :, cols], [own, core.at[t, n, :, cols]], half)
            if n < 2:
                send(t, i, summed.at[t, n, :, cols], n, qa)

    def second(t, i):
        cols = span(t, i)
        sends[t, i, 0].wait_recv()
        total(core.at[t, 0, :, cols], [summed.at[t, 2, :, cols], got.at[t, 0, :, cols]], half)
        send(t, i, core.at[t, 0, :, cols], 2, qb)

    def finish(t, i):
        cols = span(t, i)
        sends[t, i, 1].wait_recv()
        sends[t, i, 2].wait_recv()
        there = finals[t].at[mine, cols]
        total(there, [summed.at[t, 3, :, cols], got.at[t, 1, :, cols], got.at[t, 2, :, cols]], half)
        copy = remote(there, there, e_s.at[t, i], e_r.at[t, i], tp=1 - c)
        copy.start()
        ends.append(copy)

    stages = (to_core, join, second, finish)

    def step(t, i, *which):
        for s in which:
            if 0 <= i - s < nz:
                stages[s](t, i - s)

    partner, far = [], {}

    def pass_on(i, owner, kind):
        there = ts[i].at[owner, mine, :]
        copy = remote(there, there, p_s.at[i, kind], p_r.at[i, kind], tp=1 - c)
        copy.start()
        partner.append(copy)

    def adjacent(i):
        near[i, 0].wait_recv()
        there = ts[i].at[qa, mine, :]
        copy = remote(there, there, n_s.at[i, 2], n_r.at[i, 2], fs=base + qb)
        copy.start()
        far[i] = copy
        pass_on(i, qa, 0)
        near[i, 1].wait_recv()
        pass_on(i, qb, 1)

    def opposite(i):
        far[i].wait_recv()
        pass_on(i, qd, 2)

    def complete(i):
        for kind, owner in enumerate((qb, qa, qd)):
            there = ts[i].at[owner, other, :]
            remote(there, there, p_s.at[i, kind], p_r.at[i, kind], tp=1 - c).wait_recv()
        local[3 + i].wait()

    for k in range(2):
        for d, peer in enumerate((qa, qb, qd)):
            weights[k, d].wait_recv()
            along(k, landing(k, base + peer), base + peer)
        local[k].wait()
    adjacent(1)
    if nz > 2:
        relay(0, 0)
        relay(1, 0)
    adjacent(0)
    for d in range(3):
        weights[2, d].wait_recv()
    local[2].wait()
    for s in range(1, nz - 2):
        relay(0, s)
        relay(1, s)
    onward(2, 0, begin)
    adjacent(2)
    opposite(1)
    opposite(0)
    complete(1)
    for s in range(nz - 1):
        ended(0, s)
        ended(1, s)
    forward(t1, True)
    if nz > 2:
        relay(2, 0)
    opposite(2)
    complete(2)
    down_grad()
    complete(0)
    forward(t0, False)
    for s in range(1, nz - 2):
        relay(2, s)

    for i in range(nz):
        if i == nz - 1 and nz > 2:
            chain(0)
        if i > 0:
            ended(2, i - 1)
        late_block(i)
        step(0, i, 0, 1, 2)
    backward()
    step(0, nz, 1, 2)
    early_block(0)
    step(1, 0, 0)
    step(0, nz + 1, 2)
    for i in range(1, nz):
        early_block(i)
        step(1, i, 0, 1)
    for j in range(1, nz - 2):
        chain(j)
    for i in range(nz):
        finish(0, i)
    step(1, nz, 1)
    for i in range(nz):
        second(1, i)
        if i == min(1, nz - 1):
            if nz > 1:
                chain(nz - 2)
            home = gp.at[:, at(z * wide, wide)]
            if nz == 1:
                total(gsum, [home], u)
            else:
                lo_in, hi_in = gin_r.at[nz - 2], gin_l.at[nz - 2]
                for cond, srcs in ((low, [home, hi_in]), (high, [home, lo_in]),
                                   (jnp.logical_and(first, last), [home, lo_in, hi_in])):
                    @pl.when(cond)
                    def _(srcs=srcs):
                        total(gsum, srcs, u)
            handed = []
            for d, peer in enumerate((qa, qb, qd)):
                copy = remote(gsum.at[:, at(peer * r, r)], hand.at[at(q * u, u), :], g_s.at[d], g_r.at[d],
                              fs=base + peer)
                copy.start()
                handed.append(copy)
            hand[at(q * u, u), :] = gsum[:, at(q * r, r)]
        if i > 0:
            finish(1, i - 1)
    finish(1, nz - 1)
    for copy in handed:
        copy.wait_recv()

    @pl.loop(0, GROUP * u, step=128)
    def _(i):
        sl = at(i, 128)
        g[sl, :] = gd[sl, :] + hand[sl, :].astype(jnp.float32)

    for copy in ends:
        copy.wait_recv()
    for copies in (weights, near, far, cores, sends):
        for copy in copies.values():
            copy.wait_send()
    for copy in partner + handed + ends:
        copy.wait_send()
    for s in range(nz - 1):
        for k in range(3):
            onward(k, s, sent)
    for m in range(nz - 1):
        chunk = gp.at[:, at(0, wide)]

        @pl.when(jnp.logical_and(last, z <= m))
        def _():
            remote(chunk, gin_r.at[m], zr_s.at[m], zr_r.at[m], fs=f + GROUP).wait_send()

        @pl.when(jnp.logical_and(first, nz - 1 - z <= m))
        def _():
            remote(chunk, gin_l.at[m], zl_s.at[m], zl_r.at[m], fs=f - GROUP).wait_send()


def layer(nz, xs, w_gate, w_up, w_down, taps, bias, grad_down):
    rows, d = xs[0].shape
    u = w_gate.shape[1] // GROUP
    r = w_gate.shape[0]
    half, toks, wide = rows // 2, GROUP * rows, GROUP * r
    tile = 256 if u % 256 == 0 else 128
    sems = lambda *shape: [pltpu.SemaphoreType.DMA(shape)] * 2
    b16, f32 = jnp.bfloat16, jnp.float32
    out = jax.ShapeDtypeStruct((rows, d), b16)
    hops = max(nz - 1, 1)
    return pl.pallas_call(
        functools.partial(layer_kernel, nz, tile),
        out_shape=(out, out, jax.ShapeDtypeStruct((u * GROUP, r), f32)),
        in_specs=[VMEM] * 9,
        out_specs=(VMEM,) * 3,
        scratch_shapes=[pltpu.VMEM((GROUP, rows, d), b16)] * 3
        + [pltpu.VMEM((d, u), b16)] * 2
        + [pltpu.VMEM((u, d), b16), pltpu.VMEM((toks, u), b16), pltpu.VMEM((u, toks), b16),
           pltpu.VMEM((toks, u), f32), pltpu.VMEM((toks, u), f32),
           pltpu.VMEM((toks, u), b16), pltpu.VMEM((toks, u), b16),
           pltpu.VMEM((toks, d), b16), pltpu.VMEM((toks, d), b16), pltpu.VMEM((u, d), b16),
           pltpu.VMEM((2, 4, half, d), b16), pltpu.VMEM((2, 4, half, d), b16), pltpu.VMEM((2, 3, half, d), b16),
           pltpu.VMEM((hops, u, wide), b16), pltpu.VMEM((hops, u, wide), b16),
           pltpu.VMEM((u, wide), b16), pltpu.VMEM((u * GROUP, r), b16),
           pltpu.SemaphoreType.DMA((6,))]
        + sems(3, 3) + sems(3, 3) + sems(3, 3) + sems(hops, 3) + sems(hops, 3)
        + sems(2, nz, 4) + sems(2, nz, 3) + sems(hops) + sems(hops) + sems(3) + sems(2, nz),
        compiler_params=pltpu.CompilerParams(collective_id=0, has_side_effects=True, vmem_limit_bytes=VMEM_BYTES),
        name="layer_group",
    )(*xs, w_gate, w_up, w_down, taps, bias, grad_down)


def shift_later(field, steps):
    pad = jnp.zeros((steps, field.shape[1]), jnp.float32)
    return jnp.concatenate([pad, field[: field.shape[0] - steps]], axis=0)


def shift_earlier(field, steps):
    pad = jnp.zeros((steps, field.shape[1]), jnp.float32)
    return jnp.concatenate([field[steps:], pad], axis=0)


def contract_last(left, right):
    return lax.dot_general(
        left, right, (((1,), (1,)), ((), ())), preferred_element_type=jnp.float32
    )


def hidden_parts(inputs, gate_full, up_full, taps, bias):
    gate = (
        jnp.dot(inputs, gate_full, preferred_element_type=jnp.float32)
        .astype(jnp.bfloat16)
        .astype(jnp.float32)
    )
    up = jnp.dot(inputs, up_full, preferred_element_type=jnp.float32)
    conv = bias + taps[2] * gate + taps[1] * shift_later(gate, 1) + taps[0] * shift_later(gate, 2)
    act = jax.nn.silu(conv)
    hidden = (act * up).astype(jnp.bfloat16)
    return (conv, act, up, hidden)


def forward_pass(x_late, gate_full, up_full, down_full, taps, bias):
    conv, act, up, hidden = hidden_parts(x_late, gate_full, up_full, taps, bias)
    partial_value = jnp.dot(hidden, down_full, preferred_element_type=jnp.float32)
    return lax.psum(partial_value.astype(jnp.bfloat16), "tp")


def backward_pass(x_early, cotangent, gate_full, up_full, down_full, taps, bias, grad_down):
    conv, act, up, hidden = hidden_parts(x_early, gate_full, up_full, taps, bias)
    dhidden = contract_last(cotangent, down_full)
    summed = lax.psum_scatter(
        lax.dot_general(
            cotangent, hidden, (((0,), (0,)), ((), ())), preferred_element_type=jnp.float32
        ),
        "fs",
        scatter_dimension=0,
        tiled=True,
    )
    grad_down_out = grad_down + summed.T
    dup = (dhidden * act).astype(jnp.bfloat16)
    sig = jax.nn.sigmoid(conv)
    dconv = dhidden * up * sig * (1.0 + conv * (1.0 - sig))
    dgate = taps[2] * dconv + taps[1] * shift_earlier(dconv, 1) + taps[0] * shift_earlier(dconv, 2)
    dgate = dgate.astype(jnp.bfloat16)
    partial_value = contract_last(dup, up_full) + contract_last(dgate, gate_full)
    dx_early = lax.psum(partial_value.astype(jnp.bfloat16), "tp")
    return (dx_early, grad_down_out)


def shards(x_late, x_early, cotangent, w_gate, w_up, w_down, conv_taps, conv_bias, grad_down):
    width = w_gate.shape[1]
    offset = lax.axis_index("tp") * width
    taps = lax.dynamic_slice_in_dim(conv_taps, offset, width, 1)
    bias = lax.dynamic_slice_in_dim(conv_bias, offset, width, 0)
    gate_full, up_full = (
        lax.all_gather(w_gate, "fs", axis=0, tiled=True),
        lax.all_gather(w_up, "fs", axis=0, tiled=True),
    )
    down_full = lax.all_gather(w_down, "fs", axis=1, tiled=True)
    y_late = forward_pass(x_late, gate_full, up_full, down_full, taps, bias)
    dx_early, grad_down_out = backward_pass(
        x_early, cotangent, gate_full, up_full, down_full, taps, bias, grad_down
    )
    return (y_late, dx_early, grad_down_out)


def grouped_shards(nz, x_late, x_early, cotangent, w_gate, w_up, w_down, conv_taps, conv_bias, grad_down):
    return layer(
        nz, (x_late, x_early, cotangent), w_gate, w_up, w_down, conv_taps,
        conv_bias.reshape(1, conv_bias.shape[0]), grad_down,
    )


def solution(mesh):
    def step(*arrays):
        x_late, w_gate = arrays[0], arrays[3]
        fs, tp = mesh.shape["fs"], mesh.shape["tp"]
        units, rest = divmod(w_gate.shape[1], GROUP)
        lanes_ok = rest == 0 and units % 128 == 0 and w_gate.shape[0] % 128 == 0
        if tp == 2 and fs % GROUP == 0 and lanes_ok and x_late.shape[0] % 32 == 0:
            return grouped_shards(fs // GROUP, *arrays)
        return shards(*arrays)

    placed = (
        P("fs", None),
        P("fs", None),
        P("fs", None),
        P("fs", "tp"),
        P("fs", "tp"),
        P("tp", "fs"),
        P(),
        P(),
        P("tp", "fs"),
    )
    return jax.shard_map(
        step,
        mesh=mesh,
        in_specs=placed,
        out_specs=(P("fs", None), P("fs", None), P("tp", "fs")),
        check_vma=False,
    )
```

```python
import functools

import jax
import jax.numpy as jnp
from jax import lax
from jax.experimental import pallas as pl
from jax.experimental.pallas import tpu as pltpu
from jax.sharding import PartitionSpec as P

GROUP = 4
VMEM_BYTES = 63 * 1024 * 1024
VMEM = pl.BlockSpec(memory_space=pltpu.VMEM)
ANY = pl.BlockSpec(memory_space=pl.ANY)


def place():
    f, c = lax.axis_index("fs"), lax.axis_index("tp")
    q, z = lax.rem(f, GROUP), lax.div(f, GROUP)
    qx = q + 1 - 2 * lax.rem(q, 2)
    qy = q + 2 - 4 * lax.div(q, 2)
    qa, qb = qx + c * (qy - qx), qy + c * (qx - qy)
    return f, c, q, z, qa, qb, GROUP - 1 - q


def at(start, size):
    return pl.ds(pl.multiple_of(start, size), size)


def remote(src, dst, send, recv, **device):
    return pltpu.make_async_remote_copy(
        src_ref=src, dst_ref=dst, send_sem=send, recv_sem=recv,
        device_id=device, device_id_type=pl.DeviceIdType.MESH,
    )


def total(dst, srcs, rows, step=32):
    @pl.loop(0, rows, step=step)
    def _(i):
        sl = pl.ds(pl.multiple_of(i, step), step)
        out = srcs[0][sl, :].astype(jnp.float32)
        for s in srcs[1:]:
            out = out + s[sl, :].astype(jnp.float32)
        dst[sl, :] = out.astype(dst.dtype)


def mm(left, right, dims=((1,), (0,))):
    return lax.dot_general(left, right, (dims, ((), ())), preferred_element_type=jnp.float32)


def layer_kernel(nz, tile, x0, x1, x2, wg, wu, wd, taps, bias, gd_in, y_out, dx_out, g_out,
                 y, dx, g, gd, t0, t1, t2, og, ou, od, hid, hid_t, conv_s, up_s, dup, dgate, yp, xp, gp,
                 core, summed, got, gin_r, gin_l, hand, passed_r, passed_l,
                 loc, w_s, w_r, n_s, n_r, p_s, p_r, r_s, r_r, l_s, l_r,
                 c_s, c_r, a_s, a_r, zr_s, zr_r, zl_s, zl_r, g_s, g_r, pr_s, pr_r, pl_s, pl_r, fr_s, fr_r, fl_s, fl_r, e_s, e_r):
    f, c, q, z, qa, qb, qd = place()
    base = z * GROUP
    xs, ts, outs = (x0, x1, x2), (t0, t1, t2), (og, ou, od)
    rows, d_model = x0.shape
    half = rows // 2
    r, u = wg.shape[0], og.shape[1]
    wide = GROUP * r
    first, last = z > 0, z < nz - 1
    low, high = z == 0, z == nz - 1
    units = (c * GROUP + q) * u

    barrier = pltpu.get_barrier_semaphore()
    for peer in (qa, qb, qd):
        pl.semaphore_signal(barrier, 1, device_id={"fs": base + peer}, device_id_type=pl.DeviceIdType.MESH)
    pl.semaphore_signal(barrier, 1, device_id={"tp": 1 - c}, device_id_type=pl.DeviceIdType.MESH)
    for s in range(1, nz):
        for peer in range(GROUP):
            pl.semaphore_signal(barrier, 1, device_id={"fs": lax.rem(z + s, nz) * GROUP + peer},
                                device_id_type=pl.DeviceIdType.MESH)
    pl.semaphore_wait(barrier, GROUP * nz)

    def piece(k, peer):
        if k == 2:
            return wd.at[at(peer * u, u), :]
        return (wg, wu)[k].at[:, at(peer * u, u)]

    def landing(k, owner):
        if k == 2:
            return od.at[:, at(owner * r, r)]
        return outs[k].at[at(owner * r, r), :]

    def block(k, b):
        if k == 2:
            return od.at[:, at(b * wide, wide)]
        return outs[k].at[at(b * wide, wide), :]

    def right(k, s):
        b = block(k, z - s)
        return remote(b, b, r_s.at[s, k], r_r.at[s, k], fs=f + GROUP)

    def left(k, s):
        b = block(k, z + s)
        return remote(b, b, l_s.at[s, k], l_r.at[s, k], fs=f - GROUP)

    def from_left(k, s):
        b = block(k, z - s - 1)
        return remote(b, b, r_s.at[s, k], r_r.at[s, k], fs=f - GROUP)

    def from_right(k, s):
        b = block(k, z + s + 1)
        return remote(b, b, l_s.at[s, k], l_r.at[s, k], fs=f + GROUP)

    def onward(k, s, act):
        @pl.when(jnp.logical_and(z - s >= 0, last))
        def _():
            act(right(k, s))

        @pl.when(jnp.logical_and(z + s < nz, first))
        def _():
            act(left(k, s))

    begin, sent = (lambda copy: copy.start()), (lambda copy: copy.wait_send())

    def along(k, src, owner):
        there = landing(k, owner)

        @pl.when(last)
        def _():
            remote(src, there, r_s.at[0, k], r_r.at[0, k], fs=f + GROUP).start()

        @pl.when(first)
        def _():
            remote(src, there, l_s.at[0, k], l_r.at[0, k], fs=f - GROUP).start()

    def relay(k, s):
        @pl.when(jnp.logical_and(z - s - 1 >= 0, last))
        def _():
            from_left(k, s).wait_recv()
            right(k, s + 1).start()

        @pl.when(jnp.logical_and(z + s + 1 < nz, first))
        def _():
            from_right(k, s).wait_recv()
            left(k, s + 1).start()

    def ended(k, s):
        @pl.when(high)
        def _():
            from_left(k, s).wait_recv()

        @pl.when(low)
        def _():
            from_right(k, s).wait_recv()

    mine, other = at(c * half, half), at((1 - c) * half, half)
    weights, near, local = {}, {}, []

    def spread(k):
        for d, peer in enumerate((qa, qb, qd)):
            copy = remote(piece(k, peer), landing(k, f), w_s.at[k, d], w_r.at[k, d], fs=base + peer)
            copy.start()
            weights[k, d] = copy

    def share(i):
        for d, peer in enumerate((qa, qb)):
            copy = remote(xs[i].at[mine, :], ts[i].at[q, mine, :], n_s.at[i, d], n_r.at[i, d], fs=base + peer)
            copy.start()
            near[i, d] = copy

    along(0, piece(0, q), f)
    spread(0)
    along(1, piece(1, q), f)
    spread(1)
    share(1)
    share(0)
    spread(2)
    share(2)
    for k in range(3):
        copy = pltpu.make_async_copy(piece(k, q), landing(k, f), loc.at[k])
        copy.start()
        local.append(copy)
    for i in range(3):
        copy = pltpu.make_async_copy(xs[i], ts[i].at[q], loc.at[3 + i])
        copy.start()
        local.append(copy)

    old_grad = pltpu.make_async_copy(gd_in, gd, loc.at[6])
    old_grad.start()

    row = lax.broadcasted_iota(jnp.int32, (rows, tile), 0)

    def later(v, steps):
        return jnp.where(row >= steps, pltpu.roll(v, steps, 0), 0.0)

    def earlier(v, steps):
        return jnp.where(row < rows - steps, pltpu.roll(v, rows - steps, 0), 0.0)

    def forward(t, keep):
        @pl.loop(0, GROUP)
        def _(b):
            @pl.loop(0, u // tile)
            def _(j):
                cols, seq, par = at(j * tile, tile), at(b * rows, rows), at(units + j * tile, tile)
                x = t[b]
                gate = mm(x, og[:, cols]).astype(jnp.bfloat16).astype(jnp.float32)
                up = mm(x, ou[:, cols])
                conv = (bias[:, par] + taps[2:3, par] * gate + taps[1:2, par] * later(gate, 1)
                        + taps[0:1, par] * later(gate, 2))
                out = conv / (1.0 + jnp.exp(-conv)) * up
                if keep:
                    conv_s[seq, cols] = conv
                    up_s[seq, cols] = up
                    hid_t[at(j * tile, tile), seq] = out.T.astype(jnp.bfloat16)
                else:
                    hid[seq, cols] = out.astype(jnp.bfloat16)

    upper = lax.div(2 * z, nz)

    def to_owners(o, into, send_sems, recv_sems, act):
        for d, peer in enumerate((qa, qb, qd)):
            src = gp.at[:, at(o * wide + peer * r, r)]
            act(remote(src, into.at[at(q * u, u), :], send_sems.at[d], recv_sems.at[d], fs=base + peer))

    def keep_own(o, into):
        into[at(q * u, u), :] = gp[:, at(o * wide + q * r, r)]

    def exchange(act):
        to_owners(z, hand, g_s, g_r, act)

    def passing_r(act):
        to_owners(nz - 1, passed_r, pr_s, pr_r, act)

    def passing_l(act):
        to_owners(0, passed_l, pl_s, pl_r, act)

    def passed_on_r():
        return remote(passed_r, passed_r, fr_s.at[0], fr_r.at[0], fs=f + GROUP)

    def passed_on_l():
        return remote(passed_l, passed_l, fl_s.at[0], fl_r.at[0], fs=f - GROUP)

    arrival = lambda copy: copy.wait_recv()

    def hand_on():
        @pl.when(z == nz - 2)
        def _():
            passing_r(arrival)
            passed_on_r().start()

        @pl.when(z == 1)
        def _():
            passing_l(arrival)
            passed_on_l().start()

    def slot_r(o, m):
        return remote(gp.at[:, at(o * wide, wide)], gin_r.at[m], zr_s.at[m], zr_r.at[m], fs=f + GROUP)

    def slot_l(o, m):
        return remote(gp.at[:, at(o * wide, wide)], gin_l.at[m], zl_s.at[m], zl_r.at[m], fs=f - GROUP)

    def rightward(o, m, act=begin):
        if m < nz - 2:
            act(slot_r(o, m))
            return

        @pl.when(z == nz - 2)
        def _():
            passing_r(act)
            if act is begin:
                keep_own(nz - 1, passed_r)
            else:
                act(passed_on_r())

        @pl.when(z < nz - 2)
        def _():
            act(slot_r(o, m))

    def leftward(o, m, act=begin):
        if m < nz - 2:
            act(slot_l(o, m))
            return

        @pl.when(z == 1)
        def _():
            passing_l(act)
            if act is begin:
                keep_own(0, passed_l)
            else:
                act(passed_on_l())

        @pl.when(z > 1)
        def _():
            act(slot_l(o, m))

    def down_grad():
        for i in range(nz):
            o = nz - 1 - i + upper * (2 * i - (nz - 1))
            cols = at(o * wide, wide)
            cot = t2[:, :, cols].reshape(GROUP * rows, wide)
            gp[:, cols] = mm(hid_t[...], cot).astype(jnp.bfloat16)
            if i < nz - 1:
                @pl.when(low)
                def _():
                    rightward(o, i)

                @pl.when(high)
                def _():
                    leftward(o, i)

        @pl.when(jnp.logical_or(low, high))
        def _():
            exchange(begin)

    def settle():
        @pl.when(jnp.logical_and(first, last))
        def _():
            m = nz - 2
            slot_r(z, m).wait_recv()
            slot_l(z, m).wait_recv()
            home = gp.at[:, at(z * wide, wide)]
            total(home, [home, gin_r.at[m], gin_l.at[m]], u)
            exchange(begin)

    def chain(j):
        o = nz - 2 + z - j

        @pl.when(jnp.logical_and(first, o <= nz - 1))
        def _():
            slot_r(o, j).wait_recv()
            cols = at(o * wide, wide)
            total(gp.at[:, cols], [gp.at[:, cols], gin_r.at[j]], u)
            rightward(o, j + 1)

        p = z + 2 - nz + j

        @pl.when(jnp.logical_and(last, p >= 0))
        def _():
            slot_l(p, j).wait_recv()
            cols = at(p * wide, wide)
            total(gp.at[:, cols], [gp.at[:, cols], gin_l.at[j]], u)
            leftward(p, j + 1)

    def backward(b):
        @pl.loop(0, u // tile)
        def _(j):
            cols, seq, par = at(j * tile, tile), at(b * rows, rows), at(units + j * tile, tile)
            dh = mm(t2[b], od[at(j * tile, tile), :], ((1,), (1,)))
            conv = conv_s[seq, cols]
            sig = 1.0 / (1.0 + jnp.exp(-conv))
            dup[seq, cols] = (dh * (conv * sig)).astype(jnp.bfloat16)
            dc = dh * up_s[seq, cols] * sig * (1.0 + conv * (1.0 - sig))
            dg = (taps[2:3, par] * dc + taps[1:2, par] * earlier(dc, 1)
                  + taps[0:1, par] * earlier(dc, 2))
            dgate[seq, cols] = dg.astype(jnp.bfloat16)

    mirrored = z + upper * (nz - 1 - 2 * z)

    def turn(i):
        near_side = lax.div(mirrored - i + nz, nz)
        v = i + near_side * (mirrored - 2 * i)
        return v + upper * (nz - 1 - 2 * v)

    sub = 256 if wide % 256 == 0 else 128

    def late_block(i):
        start = turn(i) * wide

        @pl.loop(0, wide // sub)
        def _(j):
            cols = at(start + j * sub, sub)
            yp[:, cols] = mm(hid[...], od[:, cols]).astype(jnp.bfloat16)

    parts, finals = (yp, xp), (y, dx)
    order = (qd, qa, qb, q)
    theirs = (qd, qb, qa, q)

    def span(t, i):
        return at(turn(i) * wide, wide) if t == 0 else at(i * wide, wide)

    def core_copy(t, i, n):
        cols = span(t, i)
        src = parts[t].at[at(theirs[n] * rows + (1 - c) * half, half), cols]
        return remote(src, core.at[t, n, :, cols], c_s.at[t, i, n], c_r.at[t, i, n], tp=1 - c)

    def to_core(t, i):
        for n in range(4):
            core_copy(t, i, n).start()

    def plane_copy(t, i, slot):
        cols = span(t, i)
        src = core.at[t, 0, :, cols] if slot == 2 else summed.at[t, slot, :, cols]
        return remote(src, got.at[t, slot, :, cols], a_s.at[t, i, slot], a_r.at[t, i, slot],
                      fs=base + (qb if slot == 2 else qa))

    def join_one(t, i, n):
        cols = span(t, i)
        core_copy(t, i, n).wait_recv()
        own = parts[t].at[at(order[n] * rows + c * half, half), cols]
        total(summed.at[t, n, :, cols], [own, core.at[t, n, :, cols]], half)
        if n < 2:
            plane_copy(t, i, n).start()

    def join(t, i):
        for n in range(4):
            join_one(t, i, n)

    def second(t, i):
        cols = span(t, i)
        plane_copy(t, i, 0).wait_recv()
        total(core.at[t, 0, :, cols], [summed.at[t, 2, :, cols], got.at[t, 0, :, cols]], half)
        plane_copy(t, i, 2).start()

    def end_copy(t, i):
        there = finals[t].at[mine, span(t, i)]
        return remote(there, there, e_s.at[t, i], e_r.at[t, i], tp=1 - c)

    def finish(t, i):
        cols = span(t, i)
        plane_copy(t, i, 1).wait_recv()
        plane_copy(t, i, 2).wait_recv()
        total(finals[t].at[mine, cols], [summed.at[t, 3, :, cols], got.at[t, 1, :, cols], got.at[t, 2, :, cols]], half)
        end_copy(t, i).start()

    def each(fn):
        @pl.loop(0, nz)
        def _(i):
            fn(i)

    def early_out(owner, n):
        seq = at(owner * rows, rows)

        @pl.loop(0, nz)
        def _(i):
            cols = at(i * wide, wide)
            part = mm(dup[seq, :], ou[cols, :], ((1,), (1,))) + mm(dgate[seq, :], og[cols, :], ((1,), (1,)))
            xp[seq, cols] = part.astype(jnp.bfloat16)
            core_copy(1, i, n).start()

    def joins(n):
        each(lambda i: join_one(1, i, n))

    def seconds():
        each(lambda i: second(1, i))

    def finishes(t):
        each(lambda i: finish(t, i))

    def ended_out(t):
        each(lambda i: end_copy(t, i).wait_recv())

    stages = (to_core, join, second)

    def step(i, *which):
        for s in which:
            if 0 <= i - s < nz:
                stages[s](0, i - s)

    partner, far = [], {}

    def pass_on(i, owner, kind):
        there = ts[i].at[owner, mine, :]
        copy = remote(there, there, p_s.at[i, kind], p_r.at[i, kind], tp=1 - c)
        copy.start()
        partner.append(copy)

    def adjacent(i):
        near[i, 0].wait_recv()
        there = ts[i].at[qa, mine, :]
        copy = remote(there, there, n_s.at[i, 2], n_r.at[i, 2], fs=base + qb)
        copy.start()
        far[i] = copy
        pass_on(i, qa, 0)
        near[i, 1].wait_recv()
        pass_on(i, qb, 1)

    def opposite(i):
        far[i].wait_recv()
        pass_on(i, qd, 2)

    def complete(i):
        for kind, owner in enumerate((qb, qa, qd)):
            there = ts[i].at[owner, other, :]
            remote(there, there, p_s.at[i, kind], p_r.at[i, kind], tp=1 - c).wait_recv()
        local[3 + i].wait()

    for k in range(2):
        for d, peer in enumerate((qa, qb, qd)):
            weights[k, d].wait_recv()
            along(k, landing(k, base + peer), base + peer)
        local[k].wait()
    adjacent(1)
    if nz > 2:
        relay(0, 0)
        relay(1, 0)
    adjacent(0)
    for d in range(3):
        weights[2, d].wait_recv()
    local[2].wait()
    for s in range(1, nz - 2):
        relay(0, s)
        relay(1, s)
    onward(2, 0, begin)
    adjacent(2)
    opposite(1)
    opposite(0)
    complete(1)
    for s in range(nz - 1):
        ended(0, s)
        ended(1, s)
    forward(t1, True)
    if nz > 2:
        relay(2, 0)
    opposite(2)
    complete(2)
    down_grad()
    complete(0)
    forward(t0, False)
    for s in range(1, nz - 2):
        relay(2, s)

    for i in range(nz - 1):
        if i > 0:
            ended(2, i - 1)
        late_block(i)
        step(i, 0, 1, 2)
    step(nz - 1, 1)
    if nz > 2:
        chain(0)
    step(nz - 1, 2)
    if nz > 1:
        ended(2, nz - 2)
    late_block(nz - 1)
    to_core(0, nz - 1)
    backward(qd)
    step(nz, 1)
    early_out(qd, 0)
    step(nz, 2)
    backward(qa)
    joins(0)
    early_out(qa, 2)
    backward(qb)
    early_out(qb, 1)
    step(nz + 1, 2)
    joins(2)
    for j in range(1, nz - 2):
        chain(j)
    backward(q)
    joins(1)
    early_out(q, 3)
    seconds()
    if nz > 1:
        hand_on()
        settle()
    joins(3)
    finishes(0)
    ended_out(0)
    y_copy = pltpu.make_async_copy(y, y_out, loc.at[7])
    y_copy.start()
    finishes(1)
    exchange(arrival)
    keep_own(z, hand)
    if nz > 1:
        @pl.when(high)
        def _():
            passed_on_r().wait_recv()

        @pl.when(low)
        def _():
            passed_on_l().wait_recv()

    old_grad.wait()

    def grad_sum(*extra):
        @pl.loop(0, GROUP * u, step=128)
        def _(i):
            sl = at(i, 128)
            out = hand[sl, :].astype(jnp.float32)
            for e in extra:
                out = out + e[sl, :].astype(jnp.float32)
            g[sl, :] = gd[sl, :] + out

    inner = jnp.logical_and(first, last) if nz > 1 else low

    @pl.when(inner)
    def _():
        grad_sum()

    if nz > 1:
        @pl.when(high)
        def _():
            grad_sum(passed_r)

        @pl.when(low)
        def _():
            grad_sum(passed_l)

    g_copy = pltpu.make_async_copy(g, g_out, loc.at[8])
    g_copy.start()
    ended_out(1)
    dx_copy = pltpu.make_async_copy(dx, dx_out, loc.at[9])
    dx_copy.start()
    for copies in (weights, near, far):
        for copy in copies.values():
            copy.wait_send()
    for copy in partner:
        copy.wait_send()
    exchange(sent)
    for t in range(2):
        @pl.loop(0, nz)
        def _(i, t=t):
            for n in range(4):
                core_copy(t, i, n).wait_send()
            for slot in range(3):
                plane_copy(t, i, slot).wait_send()
            end_copy(t, i).wait_send()
    for s in range(nz - 1):
        for k in range(3):
            onward(k, s, sent)
    for m in range(nz - 2):
        @pl.when(jnp.logical_and(last, z <= m))
        def _(m=m):
            rightward(0, m, sent)

        @pl.when(jnp.logical_and(first, nz - 1 - z <= m))
        def _(m=m):
            leftward(0, m, sent)

    if nz > 1:
        @pl.when(last)
        def _():
            rightward(0, nz - 2, sent)

        @pl.when(first)
        def _():
            leftward(0, nz - 2, sent)

    for copy in (y_copy, g_copy, dx_copy):
        copy.wait()


def layer(nz, xs, w_gate, w_up, w_down, taps, bias, grad_down):
    rows, d = xs[0].shape
    u = w_gate.shape[1] // GROUP
    r = w_gate.shape[0]
    half, toks, wide = rows // 2, GROUP * rows, GROUP * r
    tile = 256 if u % 256 == 0 else 128
    sems = lambda *shape: [pltpu.SemaphoreType.DMA(shape)] * 2
    b16, f32 = jnp.bfloat16, jnp.float32
    out = jax.ShapeDtypeStruct((rows, d), b16)
    hops = max(nz - 1, 1)
    return pl.pallas_call(
        functools.partial(layer_kernel, nz, tile),
        out_shape=(out, out, jax.ShapeDtypeStruct((u * GROUP, r), f32)),
        in_specs=[ANY] * 6 + [VMEM] * 2 + [ANY],
        out_specs=(ANY,) * 3,
        scratch_shapes=[pltpu.VMEM((rows, d), b16)] * 2
        + [pltpu.VMEM((u * GROUP, r), f32)] * 2
        + [pltpu.VMEM((GROUP, rows, d), b16)] * 3
        + [pltpu.VMEM((d, u), b16)] * 2
        + [pltpu.VMEM((u, d), b16), pltpu.VMEM((toks, u), b16), pltpu.VMEM((u, toks), b16),
           pltpu.VMEM((toks, u), f32), pltpu.VMEM((toks, u), f32),
           pltpu.VMEM((toks, u), b16), pltpu.VMEM((toks, u), b16),
           pltpu.VMEM((toks, d), b16), pltpu.VMEM((toks, d), b16), pltpu.VMEM((u, d), b16),
           pltpu.VMEM((2, 4, half, d), b16), pltpu.VMEM((2, 4, half, d), b16), pltpu.VMEM((2, 3, half, d), b16),
           pltpu.VMEM((hops, u, wide), b16), pltpu.VMEM((hops, u, wide), b16)]
        + [pltpu.VMEM((u * GROUP, r), b16)] * 3
        + [pltpu.SemaphoreType.DMA((10,))]
        + sems(3, 3) + sems(3, 3) + sems(3, 3) + sems(hops, 3) + sems(hops, 3)
        + sems(2, nz, 4) + sems(2, nz, 3) + sems(hops) + sems(hops) + sems(3)
        + sems(3) + sems(3) + sems(1) + sems(1) + sems(2, nz),
        compiler_params=pltpu.CompilerParams(collective_id=0, has_side_effects=True, vmem_limit_bytes=VMEM_BYTES),
        name="layer_group",
    )(*xs, w_gate, w_up, w_down, taps, bias, grad_down)


def shift_later(field, steps):
    pad = jnp.zeros((steps, field.shape[1]), jnp.float32)
    return jnp.concatenate([pad, field[: field.shape[0] - steps]], axis=0)


def shift_earlier(field, steps):
    pad = jnp.zeros((steps, field.shape[1]), jnp.float32)
    return jnp.concatenate([field[steps:], pad], axis=0)


def contract_last(left, right):
    return lax.dot_general(
        left, right, (((1,), (1,)), ((), ())), preferred_element_type=jnp.float32
    )


def hidden_parts(inputs, gate_full, up_full, taps, bias):
    gate = (
        jnp.dot(inputs, gate_full, preferred_element_type=jnp.float32)
        .astype(jnp.bfloat16)
        .astype(jnp.float32)
    )
    up = jnp.dot(inputs, up_full, preferred_element_type=jnp.float32)
    conv = bias + taps[2] * gate + taps[1] * shift_later(gate, 1) + taps[0] * shift_later(gate, 2)
    act = jax.nn.silu(conv)
    hidden = (act * up).astype(jnp.bfloat16)
    return (conv, act, up, hidden)


def forward_pass(x_late, gate_full, up_full, down_full, taps, bias):
    conv, act, up, hidden = hidden_parts(x_late, gate_full, up_full, taps, bias)
    partial_value = jnp.dot(hidden, down_full, preferred_element_type=jnp.float32)
    return lax.psum(partial_value.astype(jnp.bfloat16), "tp")


def backward_pass(x_early, cotangent, gate_full, up_full, down_full, taps, bias, grad_down):
    conv, act, up, hidden = hidden_parts(x_early, gate_full, up_full, taps, bias)
    dhidden = contract_last(cotangent, down_full)
    summed = lax.psum_scatter(
        lax.dot_general(
            cotangent, hidden, (((0,), (0,)), ((), ())), preferred_element_type=jnp.float32
        ),
        "fs",
        scatter_dimension=0,
        tiled=True,
    )
    grad_down_out = grad_down + summed.T
    dup = (dhidden * act).astype(jnp.bfloat16)
    sig = jax.nn.sigmoid(conv)
    dconv = dhidden * up * sig * (1.0 + conv * (1.0 - sig))
    dgate = taps[2] * dconv + taps[1] * shift_earlier(dconv, 1) + taps[0] * shift_earlier(dconv, 2)
    dgate = dgate.astype(jnp.bfloat16)
    partial_value = contract_last(dup, up_full) + contract_last(dgate, gate_full)
    dx_early = lax.psum(partial_value.astype(jnp.bfloat16), "tp")
    return (dx_early, grad_down_out)


def shards(x_late, x_early, cotangent, w_gate, w_up, w_down, conv_taps, conv_bias, grad_down):
    width = w_gate.shape[1]
    offset = lax.axis_index("tp") * width
    taps = lax.dynamic_slice_in_dim(conv_taps, offset, width, 1)
    bias = lax.dynamic_slice_in_dim(conv_bias, offset, width, 0)
    gate_full, up_full = (
        lax.all_gather(w_gate, "fs", axis=0, tiled=True),
        lax.all_gather(w_up, "fs", axis=0, tiled=True),
    )
    down_full = lax.all_gather(w_down, "fs", axis=1, tiled=True)
    y_late = forward_pass(x_late, gate_full, up_full, down_full, taps, bias)
    dx_early, grad_down_out = backward_pass(
        x_early, cotangent, gate_full, up_full, down_full, taps, bias, grad_down
    )
    return (y_late, dx_early, grad_down_out)


def grouped_shards(nz, x_late, x_early, cotangent, w_gate, w_up, w_down, conv_taps, conv_bias, grad_down):
    return layer(
        nz, (x_late, x_early, cotangent), w_gate, w_up, w_down, conv_taps,
        conv_bias.reshape(1, conv_bias.shape[0]), grad_down,
    )


def solution(mesh):
    def step(*arrays):
        x_late, w_gate = arrays[0], arrays[3]
        fs, tp = mesh.shape["fs"], mesh.shape["tp"]
        units, rest = divmod(w_gate.shape[1], GROUP)
        lanes_ok = rest == 0 and units % 128 == 0 and w_gate.shape[0] % 128 == 0
        if tp == 2 and fs % GROUP == 0 and lanes_ok and x_late.shape[0] % 32 == 0:
            return grouped_shards(fs // GROUP, *arrays)
        return shards(*arrays)

    placed = (
        P("fs", None),
        P("fs", None),
        P("fs", None),
        P("fs", "tp"),
        P("fs", "tp"),
        P("tp", "fs"),
        P(),
        P(),
        P("tp", "fs"),
    )
    return jax.shard_map(
        step,
        mesh=mesh,
        in_specs=placed,
        out_specs=(P("fs", None), P("fs", None), P("tp", "fs")),
        check_vma=False,
    )
```

```python
import functools

import jax
import jax.numpy as jnp
from jax import lax
from jax.experimental import pallas as pl
from jax.experimental.pallas import tpu as pltpu
from jax.sharding import PartitionSpec as P

GROUP = 4
VMEM_BYTES = 63 * 1024 * 1024
VMEM = pl.BlockSpec(memory_space=pltpu.VMEM)
ANY = pl.BlockSpec(memory_space=pl.ANY)


def place():
    f, c = lax.axis_index("fs"), lax.axis_index("tp")
    q, z = lax.rem(f, GROUP), lax.div(f, GROUP)
    qx = q + 1 - 2 * lax.rem(q, 2)
    qy = q + 2 - 4 * lax.div(q, 2)
    qa, qb = qx + c * (qy - qx), qy + c * (qx - qy)
    return f, c, q, z, qa, qb, GROUP - 1 - q


def at(start, size):
    return pl.ds(pl.multiple_of(start, size), size)


def remote(src, dst, send, recv, **device):
    return pltpu.make_async_remote_copy(
        src_ref=src, dst_ref=dst, send_sem=send, recv_sem=recv,
        device_id=device, device_id_type=pl.DeviceIdType.MESH,
    )


def total(dst, srcs, rows, step=32):
    @pl.loop(0, rows, step=step)
    def _(i):
        sl = pl.ds(pl.multiple_of(i, step), step)
        out = srcs[0][sl, :].astype(jnp.float32)
        for s in srcs[1:]:
            out = out + s[sl, :].astype(jnp.float32)
        dst[sl, :] = out.astype(dst.dtype)


def mm(left, right, dims=((1,), (0,))):
    return lax.dot_general(left, right, (dims, ((), ())), preferred_element_type=jnp.float32)


def layer_kernel(nz, tile, x0, x1, x2, wg, wu, wd, taps, bias, gd_in, y_out, dx_out, g_out,
                 y, dx, g, gd, t0, t1, t2, og, ou, od, hid, hid_t, conv_s, up_s, gate_l, up_l, dup, dgate, yp, xp, gp,
                 core, summed, got, gin_r, gin_l, hand, passed_r, passed_l,
                 loc, w_s, w_r, n_s, n_r, p_s, p_r, r_s, r_r, l_s, l_r,
                 c_s, c_r, a_s, a_r, zr_s, zr_r, zl_s, zl_r, g_s, g_r, pr_s, pr_r, pl_s, pl_r, fr_s, fr_r, fl_s, fl_r, e_s, e_r, o_s):
    f, c, q, z, qa, qb, qd = place()
    base = z * GROUP
    xs, ts, outs = (x0, x1, x2), (t0, t1, t2), (og, ou, od)
    rows, d_model = x0.shape
    half = rows // 2
    r, u = wg.shape[0], og.shape[1]
    wide = GROUP * r
    parts_d = wide // 256 if wide % 256 == 0 else 1
    part, downs = wide // parts_d, range(2, 2 + parts_d)
    first, last = z > 0, z < nz - 1
    low, high = z == 0, z == nz - 1
    units = (c * GROUP + q) * u

    barrier = pltpu.get_barrier_semaphore()
    for peer in (qa, qb, qd):
        pl.semaphore_signal(barrier, 1, device_id={"fs": base + peer}, device_id_type=pl.DeviceIdType.MESH)
    pl.semaphore_signal(barrier, 1, device_id={"tp": 1 - c}, device_id_type=pl.DeviceIdType.MESH)
    @pl.when(last)
    def _():
        pl.semaphore_signal(barrier, 1, device_id={"fs": f + GROUP}, device_id_type=pl.DeviceIdType.MESH)

    @pl.when(first)
    def _():
        pl.semaphore_signal(barrier, 1, device_id={"fs": f - GROUP}, device_id_type=pl.DeviceIdType.MESH)

    beside = lax.div(z + nz - 1, nz) + lax.div(2 * nz - 2 - z, nz)
    pl.semaphore_wait(barrier, GROUP + beside)

    def piece(k, peer):
        if k == 2:
            return wd.at[at(peer * u, u), :]
        return (wg, wu)[k].at[:, at(peer * u, u)]

    def landing(k, owner):
        if k == 2:
            return od.at[:, at(owner * r, r)]
        return outs[k].at[at(owner * r, r), :]

    def block(k, b):
        if k >= 2:
            return od.at[:, at(b * wide + (k - 2) * part, part)]
        return outs[k].at[at(b * wide, wide), :]

    def right(k, s):
        b = block(k, z - s)
        return remote(b, b, r_s.at[s, k], r_r.at[s, k], fs=f + GROUP)

    def left(k, s):
        b = block(k, z + s)
        return remote(b, b, l_s.at[s, k], l_r.at[s, k], fs=f - GROUP)

    def from_left(k, s):
        b = block(k, z - s - 1)
        return remote(b, b, r_s.at[s, k], r_r.at[s, k], fs=f - GROUP)

    def from_right(k, s):
        b = block(k, z + s + 1)
        return remote(b, b, l_s.at[s, k], l_r.at[s, k], fs=f + GROUP)

    def onward(k, s, act):
        @pl.when(jnp.logical_and(z - s >= 0, last))
        def _():
            act(right(k, s))

        @pl.when(jnp.logical_and(z + s < nz, first))
        def _():
            act(left(k, s))

    begin, sent = (lambda copy: copy.start()), (lambda copy: copy.wait_send())

    def along(k, src, owner):
        there = landing(k, owner)

        @pl.when(last)
        def _():
            remote(src, there, r_s.at[0, k], r_r.at[0, k], fs=f + GROUP).start()

        @pl.when(first)
        def _():
            remote(src, there, l_s.at[0, k], l_r.at[0, k], fs=f - GROUP).start()

    def relay(k, s):
        @pl.when(jnp.logical_and(z - s - 1 >= 0, last))
        def _():
            from_left(k, s).wait_recv()
            right(k, s + 1).start()

        @pl.when(jnp.logical_and(z + s + 1 < nz, first))
        def _():
            from_right(k, s).wait_recv()
            left(k, s + 1).start()

    def ended(k, s):
        @pl.when(high)
        def _():
            from_left(k, s).wait_recv()

        @pl.when(low)
        def _():
            from_right(k, s).wait_recv()

    mine, other = at(c * half, half), at((1 - c) * half, half)
    weights, near, local = {}, {}, []

    def spread(k):
        for d, peer in enumerate((qa, qb, qd)):
            copy = remote(piece(k, peer), landing(k, f), w_s.at[k, d], w_r.at[k, d], fs=base + peer)
            copy.start()
            weights[k, d] = copy

    def share(i):
        for d, peer in enumerate((qa, qb)):
            copy = remote(xs[i].at[mine, :], ts[i].at[q, mine, :], n_s.at[i, d], n_r.at[i, d], fs=base + peer)
            copy.start()
            near[i, d] = copy

    along(0, piece(0, q), f)
    spread(0)
    along(1, piece(1, q), f)
    spread(1)
    share(1)
    share(0)
    spread(2)
    share(2)
    for k in range(3):
        copy = pltpu.make_async_copy(piece(k, q), landing(k, f), loc.at[k])
        copy.start()
        local.append(copy)
    for i in range(3):
        copy = pltpu.make_async_copy(xs[i], ts[i].at[q], loc.at[3 + i])
        copy.start()
        local.append(copy)

    old_grad = pltpu.make_async_copy(gd_in, gd, loc.at[6])
    old_grad.start()

    row = lax.broadcasted_iota(jnp.int32, (rows, tile), 0)

    def later(v, steps):
        return jnp.where(row >= steps, pltpu.roll(v, steps, 0), 0.0)

    def earlier(v, steps):
        return jnp.where(row < rows - steps, pltpu.roll(v, rows - steps, 0), 0.0)

    upper = lax.div(2 * z, nz)
    head_k = pl.ds(pl.multiple_of(upper * wide, wide), max(nz - 1, 1) * wide)
    tail_k = at((1 - upper) * (nz - 1) * wide, wide)

    def begun(i):
        t, kept_gate, kept_up = ((t0, gate_l, up_l), (t1, conv_s, up_s))[i]

        @pl.loop(0, GROUP)
        def _(b):
            @pl.loop(0, u // tile)
            def _(j):
                cols, seq = at(j * tile, tile), at(b * rows, rows)
                x = t[b, :, head_k]
                kept_gate[seq, cols] = mm(x, og[head_k, cols])
                kept_up[seq, cols] = mm(x, ou[head_k, cols])

    def forward(i, split):
        t, kept_gate, kept_up = ((t0, gate_l, up_l), (t1, conv_s, up_s))[i]
        keep = i == 1

        @pl.loop(0, GROUP)
        def _(b):
            @pl.loop(0, u // tile)
            def _(j):
                cols, seq, par = at(j * tile, tile), at(b * rows, rows), at(units + j * tile, tile)
                if split:
                    x = t[b, :, tail_k]
                    gate = kept_gate[seq, cols] + mm(x, og[tail_k, cols])
                    up = kept_up[seq, cols] + mm(x, ou[tail_k, cols])
                else:
                    x = t[b]
                    gate, up = mm(x, og[:, cols]), mm(x, ou[:, cols])
                gate = gate.astype(jnp.bfloat16).astype(jnp.float32)
                conv = (bias[:, par] + taps[2:3, par] * gate + taps[1:2, par] * later(gate, 1)
                        + taps[0:1, par] * later(gate, 2))
                out = conv / (1.0 + jnp.exp(-conv)) * up
                if keep:
                    conv_s[seq, cols] = conv
                    up_s[seq, cols] = up
                    hid_t[at(j * tile, tile), seq] = out.T.astype(jnp.bfloat16)
                else:
                    hid[seq, cols] = out.astype(jnp.bfloat16)

    def to_owners(o, into, send_sems, recv_sems, act):
        for d, peer in enumerate((qa, qb, qd)):
            src = gp.at[:, at(o * wide + peer * r, r)]
            act(remote(src, into.at[at(q * u, u), :], send_sems.at[d], recv_sems.at[d], fs=base + peer))

    def keep_own(o, into):
        into[at(q * u, u), :] = gp[:, at(o * wide + q * r, r)]

    def exchange(act):
        to_owners(z, hand, g_s, g_r, act)

    def passing_r(act):
        to_owners(nz - 1, passed_r, pr_s, pr_r, act)

    def passing_l(act):
        to_owners(0, passed_l, pl_s, pl_r, act)

    def passed_on_r():
        return remote(passed_r, passed_r, fr_s.at[0], fr_r.at[0], fs=f + GROUP)

    def passed_on_l():
        return remote(passed_l, passed_l, fl_s.at[0], fl_r.at[0], fs=f - GROUP)

    arrival = lambda copy: copy.wait_recv()

    def hand_on():
        @pl.when(z == nz - 2)
        def _():
            passing_r(arrival)
            passed_on_r().start()

        @pl.when(z == 1)
        def _():
            passing_l(arrival)
            passed_on_l().start()

    def slot_r(o, m):
        return remote(gp.at[:, at(o * wide, wide)], gin_r.at[m], zr_s.at[m], zr_r.at[m], fs=f + GROUP)

    def slot_l(o, m):
        return remote(gp.at[:, at(o * wide, wide)], gin_l.at[m], zl_s.at[m], zl_r.at[m], fs=f - GROUP)

    def rightward(o, m, act=begin):
        if m < nz - 2:
            act(slot_r(o, m))
            return

        @pl.when(z == nz - 2)
        def _():
            passing_r(act)
            if act is begin:
                keep_own(nz - 1, passed_r)
            else:
                act(passed_on_r())

        @pl.when(z < nz - 2)
        def _():
            act(slot_r(o, m))

    def leftward(o, m, act=begin):
        if m < nz - 2:
            act(slot_l(o, m))
            return

        @pl.when(z == 1)
        def _():
            passing_l(act)
            if act is begin:
                keep_own(0, passed_l)
            else:
                act(passed_on_l())

        @pl.when(z > 1)
        def _():
            act(slot_l(o, m))

    def down_grad():
        for i in range(nz):
            o = nz - 1 - i + upper * (2 * i - (nz - 1))
            cols = at(o * wide, wide)
            cot = t2[:, :, cols].reshape(GROUP * rows, wide)
            gp[:, cols] = mm(hid_t[...], cot).astype(jnp.bfloat16)
            if i < nz - 1:
                @pl.when(low)
                def _():
                    rightward(o, i)

                @pl.when(high)
                def _():
                    leftward(o, i)

        @pl.when(jnp.logical_or(low, high))
        def _():
            exchange(begin)

    def settle():
        @pl.when(jnp.logical_and(first, last))
        def _():
            m = nz - 2
            slot_r(z, m).wait_recv()
            slot_l(z, m).wait_recv()
            home = gp.at[:, at(z * wide, wide)]
            total(home, [home, gin_r.at[m], gin_l.at[m]], u)
            exchange(begin)

    def chain(j):
        o = nz - 2 + z - j

        @pl.when(jnp.logical_and(first, o <= nz - 1))
        def _():
            slot_r(o, j).wait_recv()
            cols = at(o * wide, wide)
            total(gp.at[:, cols], [gp.at[:, cols], gin_r.at[j]], u)
            rightward(o, j + 1)

        p = z + 2 - nz + j

        @pl.when(jnp.logical_and(last, p >= 0))
        def _():
            slot_l(p, j).wait_recv()
            cols = at(p * wide, wide)
            total(gp.at[:, cols], [gp.at[:, cols], gin_l.at[j]], u)
            leftward(p, j + 1)

    def backward(n):
        b, out = order[n], pl.ds(n * rows, rows)

        @pl.loop(0, u // tile)
        def _(j):
            cols, seq, par = at(j * tile, tile), at(b * rows, rows), at(units + j * tile, tile)
            dh = mm(t2[b], od[at(j * tile, tile), :], ((1,), (1,)))
            conv = conv_s[seq, cols]
            sig = 1.0 / (1.0 + jnp.exp(-conv))
            dup[out, cols] = (dh * (conv * sig)).astype(jnp.bfloat16)
            dc = dh * up_s[seq, cols] * sig * (1.0 + conv * (1.0 - sig))
            dg = (taps[2:3, par] * dc + taps[1:2, par] * earlier(dc, 1)
                  + taps[0:1, par] * earlier(dc, 2))
            dgate[out, cols] = dg.astype(jnp.bfloat16)

    mirrored = z + upper * (nz - 1 - 2 * z)

    def turn(i):
        near_side = lax.div(mirrored - i + nz, nz)
        v = i + near_side * (mirrored - 2 * i)
        return v + upper * (nz - 1 - 2 * v)


    def late_start(h):
        return turn(h // parts_d) * wide + h % parts_d * part if isinstance(h, int) else (
            turn(lax.div(h, parts_d)) * wide + lax.rem(h, parts_d) * part)

    def late_block(h):
        cols = at(late_start(h), part)
        yp[:, cols] = mm(hid[...], od[:, cols]).astype(jnp.bfloat16)

    parts, finals, results = (yp, xp), (y, dx), (y_out, dx_out)
    order = (qd, qa, qb, q)
    theirs = (qd, qb, qa, q)
    places = ((order, theirs), ((0, 1, 2, 3), (0, 2, 1, 3)))

    def span(t, i):
        return at(late_start(i), part) if t == 0 else at(i * wide, wide)

    def core_copy(t, i, n):
        cols = span(t, i)
        src = parts[t].at[at(places[t][1][n] * rows + (1 - c) * half, half), cols]
        return remote(src, core.at[t, n, :, cols], c_s.at[t, i, n], c_r.at[t, i, n], tp=1 - c)

    def to_core(t, i):
        for n in range(4):
            core_copy(t, i, n).start()

    def plane_copy(t, i, slot):
        cols = span(t, i)
        src = core.at[t, 0, :, cols] if slot == 2 else summed.at[t, slot, :, cols]
        return remote(src, got.at[t, slot, :, cols], a_s.at[t, i, slot], a_r.at[t, i, slot],
                      fs=base + (qb if slot == 2 else qa))

    def join_one(t, i, n):
        cols = span(t, i)
        core_copy(t, i, n).wait_recv()
        own = parts[t].at[at(places[t][0][n] * rows + c * half, half), cols]
        total(summed.at[t, n, :, cols], [own, core.at[t, n, :, cols]], half)
        if n < 2:
            plane_copy(t, i, n).start()

    def join(t, i):
        for n in range(4):
            join_one(t, i, n)

    def second(t, i):
        cols = span(t, i)
        plane_copy(t, i, 0).wait_recv()
        total(core.at[t, 0, :, cols], [summed.at[t, 2, :, cols], got.at[t, 0, :, cols]], half)
        plane_copy(t, i, 2).start()

    def end_copy(t, i):
        cols = span(t, i)
        return remote(finals[t].at[:, cols], results[t].at[mine, cols], e_s.at[t, i], e_r.at[t, i], tp=1 - c)

    def own_copy(t, i):
        cols = span(t, i)
        return pltpu.make_async_copy(finals[t].at[:, cols], results[t].at[mine, cols], o_s.at[t, i])

    def finish(t, i):
        cols = span(t, i)
        plane_copy(t, i, 1).wait_recv()
        plane_copy(t, i, 2).wait_recv()
        total(finals[t].at[:, cols], [summed.at[t, 3, :, cols], got.at[t, 1, :, cols], got.at[t, 2, :, cols]], half)
        end_copy(t, i).start()
        own_copy(t, i).start()

    blocks = (nz * parts_d, nz)

    def each(fn, t=1):
        @pl.loop(0, blocks[t])
        def _(i):
            fn(i)

    def early_piece(n, m, i):
        seq, cols = pl.ds(n * rows, m * rows), at(i * wide, wide)
        out = mm(dup[seq, :], ou[cols, :], ((1,), (1,))) + mm(dgate[seq, :], og[cols, :], ((1,), (1,)))
        xp[seq, cols] = out.astype(jnp.bfloat16)
        for k in range(n, n + m):
            core_copy(1, i, (0, 2, 1, 3)[k]).start()

    def first_out():
        for i in range(nz + 2):
            if i < nz:
                early_piece(0, 1, i)
            if i > 1:
                join_one(1, i - 2, 0)

    def pair_out():
        for i in range(nz + 1):
            if i < nz:
                early_piece(1, 2, i)
            if i > 0:
                join_one(1, i - 1, 2)
                join_one(1, i - 1, 1)
            if 1 < i < nz:
                second(1, i - 2)

    def last_out():
        each(lambda i: early_piece(3, 1, i))

    def joins(n):
        each(lambda i: join_one(1, i, n))

    def finishes(t):
        each(lambda i: finish(t, i), t)

    def ended_out(t):
        each(lambda i: end_copy(t, i).wait_recv(), t)

    partner, far = [], {}

    def pass_on(i, owner, kind):
        there = ts[i].at[owner, mine, :]
        copy = remote(there, there, p_s.at[i, kind], p_r.at[i, kind], tp=1 - c)
        copy.start()
        partner.append(copy)

    def adjacent(i):
        near[i, 0].wait_recv()
        there = ts[i].at[qa, mine, :]
        copy = remote(there, there, n_s.at[i, 2], n_r.at[i, 2], fs=base + qb)
        copy.start()
        far[i] = copy
        pass_on(i, qa, 0)
        near[i, 1].wait_recv()
        pass_on(i, qb, 1)

    def opposite(i):
        far[i].wait_recv()
        pass_on(i, qd, 2)

    def complete(i):
        for kind, owner in enumerate((qb, qa, qd)):
            there = ts[i].at[owner, other, :]
            remote(there, there, p_s.at[i, kind], p_r.at[i, kind], tp=1 - c).wait_recv()
        local[3 + i].wait()

    for k in range(2):
        for d, peer in enumerate((qa, qb, qd)):
            weights[k, d].wait_recv()
            along(k, landing(k, base + peer), base + peer)
        local[k].wait()
    adjacent(1)
    if nz > 2:
        relay(0, 0)
        relay(1, 0)
    adjacent(0)
    for d in range(3):
        weights[2, d].wait_recv()
    local[2].wait()
    for s in range(1, nz - 2):
        relay(0, s)
        relay(1, s)
    for k in downs:
        onward(k, 0, begin)
    adjacent(2)
    at_end = jnp.logical_or(low, high) if nz > 1 else z < 0
    inside = jnp.logical_and(first, last) if nz > 1 else z >= 0

    def forward_head(i):
        @pl.when(at_end)
        def _():
            begun(i)

        @pl.when(inside)
        def _():
            forward(i, False)

    def forward_tail(i):
        @pl.when(at_end)
        def _():
            forward(i, True)

    opposite(1)
    complete(1)
    for s in range(nz - 2):
        ended(0, s)
        ended(1, s)
    if nz > 2:
        for k in downs:
            relay(k, 0)
    forward_head(1)
    opposite(0)
    complete(0)
    forward_head(0)
    for s in range(1, nz - 2):
        for k in downs:
            relay(k, s)
    if nz > 1:
        ended(0, nz - 2)
        ended(1, nz - 2)
    forward_tail(1)
    opposite(2)
    complete(2)
    down_grad()
    forward_tail(0)

    count = blocks[0]

    @pl.when(at_end)
    def _():
        progress = [0, 0]

        def catch_up(stage, upto):
            while progress[stage] <= upto:
                (join, second)[stage](0, progress[stage])
                progress[stage] += 1

        for h in range(count - 1):
            i, p = divmod(h, parts_d)
            if i > 0:
                ended(2 + p, i - 1)
            late_block(h)
            to_core(0, h)
            if h > 2:
                catch_up(1, h - 3)
            catch_up(0, h - 1)
            if h == parts_d * (nz - 2) - 1:
                catch_up(0, h)
                catch_up(1, h - 1)
        catch_up(0, count - 2)
        catch_up(1, count - 4)
        if nz > 1:
            ended(1 + parts_d, nz - 2)
        late_block(count - 1)
        to_core(0, count - 1)

    @pl.when(inside)
    def _():
        for h in range(count):
            late_block(h)
            to_core(0, h)
            if h > 1:
                join(0, h - 2)
        for h in range(max(count - 2, 0), count - 1):
            join(0, h)

    def seconds_late(begin_at):
        @pl.loop(begin_at, count)
        def _(h):
            second(0, h)

    backward(0)
    join(0, count - 1)
    first_out()
    if nz > 2:
        chain(0)

    @pl.when(at_end)
    def _():
        seconds_late(max(count - 3, 0))

    @pl.when(inside)
    def _():
        seconds_late(0)

    backward(1)
    backward(2)
    for j in range(1, nz - 2):
        chain(j)
    pair_out()
    if nz > 1:
        hand_on()
    for i in range(max(nz - 2, 0), nz):
        second(1, i)
    backward(3)
    last_out()
    joins(3)
    if nz > 1:
        settle()
    finishes(0)
    finishes(1)
    exchange(arrival)
    keep_own(z, hand)
    if nz > 1:
        @pl.when(high)
        def _():
            passed_on_r().wait_recv()

        @pl.when(low)
        def _():
            passed_on_l().wait_recv()

    old_grad.wait()

    def grad_sum(*extra):
        @pl.loop(0, GROUP * u, step=128)
        def _(i):
            sl = at(i, 128)
            out = hand[sl, :].astype(jnp.float32)
            for e in extra:
                out = out + e[sl, :].astype(jnp.float32)
            g[sl, :] = gd[sl, :] + out

    @pl.when(inside)
    def _():
        grad_sum()

    if nz > 1:
        @pl.when(high)
        def _():
            grad_sum(passed_r)

        @pl.when(low)
        def _():
            grad_sum(passed_l)

    g_copy = pltpu.make_async_copy(g, g_out, loc.at[8])
    g_copy.start()
    for t in range(2):
        ended_out(t)
    for copies in (weights, near, far):
        for copy in copies.values():
            copy.wait_send()
    for copy in partner:
        copy.wait_send()
    exchange(sent)
    for t in range(2):
        @pl.loop(0, blocks[t])
        def _(i, t=t):
            for n in range(4):
                core_copy(t, i, n).wait_send()
            for slot in range(3):
                plane_copy(t, i, slot).wait_send()
            end_copy(t, i).wait_send()
            own_copy(t, i).wait()
    for s in range(nz - 1):
        for k in range(2 + parts_d):
            onward(k, s, sent)
    for m in range(nz - 2):
        @pl.when(jnp.logical_and(last, z <= m))
        def _(m=m):
            rightward(0, m, sent)

        @pl.when(jnp.logical_and(first, nz - 1 - z <= m))
        def _(m=m):
            leftward(0, m, sent)

    if nz > 1:
        @pl.when(last)
        def _():
            rightward(0, nz - 2, sent)

        @pl.when(first)
        def _():
            leftward(0, nz - 2, sent)

    g_copy.wait()


def layer(nz, xs, w_gate, w_up, w_down, taps, bias, grad_down):
    rows, d = xs[0].shape
    u = w_gate.shape[1] // GROUP
    r = w_gate.shape[0]
    half, toks, wide = rows // 2, GROUP * rows, GROUP * r
    tile = 256 if u % 256 == 0 else 128
    sems = lambda *shape: [pltpu.SemaphoreType.DMA(shape)] * 2
    b16, f32 = jnp.bfloat16, jnp.float32
    out = jax.ShapeDtypeStruct((rows, d), b16)
    hops = max(nz - 1, 1)
    parts_d = wide // 256 if wide % 256 == 0 else 1
    count = nz * parts_d
    return pl.pallas_call(
        functools.partial(layer_kernel, nz, tile),
        out_shape=(out, out, jax.ShapeDtypeStruct((u * GROUP, r), f32)),
        in_specs=[ANY] * 6 + [VMEM] * 2 + [ANY],
        out_specs=(ANY,) * 3,
        scratch_shapes=[pltpu.VMEM((half, d), b16)] * 2
        + [pltpu.VMEM((u * GROUP, r), f32)] * 2
        + [pltpu.VMEM((GROUP, rows, d), b16)] * 3
        + [pltpu.VMEM((d, u), b16)] * 2
        + [pltpu.VMEM((u, d), b16), pltpu.VMEM((toks, u), b16), pltpu.VMEM((u, toks), b16),
           pltpu.VMEM((toks, u), f32), pltpu.VMEM((toks, u), f32),
           pltpu.VMEM((toks, u), f32), pltpu.VMEM((toks, u), f32),
           pltpu.VMEM((toks, u), b16), pltpu.VMEM((toks, u), b16),
           pltpu.VMEM((toks, d), b16), pltpu.VMEM((toks, d), b16), pltpu.VMEM((u, d), b16),
           pltpu.VMEM((2, 4, half, d), b16), pltpu.VMEM((2, 4, half, d), b16), pltpu.VMEM((2, 3, half, d), b16),
           pltpu.VMEM((hops, u, wide), b16), pltpu.VMEM((hops, u, wide), b16)]
        + [pltpu.VMEM((u * GROUP, r), b16)] * 3
        + [pltpu.SemaphoreType.DMA((10,))]
        + sems(3, 3) + sems(3, 3) + sems(3, 3) + sems(hops, 2 + parts_d) + sems(hops, 2 + parts_d)
        + sems(2, count, 4) + sems(2, count, 3) + sems(hops) + sems(hops) + sems(3)
        + sems(3) + sems(3) + sems(1) + sems(1) + sems(2, count)
        + [pltpu.SemaphoreType.DMA((2, count))],
        compiler_params=pltpu.CompilerParams(collective_id=0, has_side_effects=True, vmem_limit_bytes=VMEM_BYTES),
        name="layer_group",
    )(*xs, w_gate, w_up, w_down, taps, bias, grad_down)


def shift_later(field, steps):
    pad = jnp.zeros((steps, field.shape[1]), jnp.float32)
    return jnp.concatenate([pad, field[: field.shape[0] - steps]], axis=0)


def shift_earlier(field, steps):
    pad = jnp.zeros((steps, field.shape[1]), jnp.float32)
    return jnp.concatenate([field[steps:], pad], axis=0)


def contract_last(left, right):
    return lax.dot_general(
        left, right, (((1,), (1,)), ((), ())), preferred_element_type=jnp.float32
    )


def hidden_parts(inputs, gate_full, up_full, taps, bias):
    gate = (
        jnp.dot(inputs, gate_full, preferred_element_type=jnp.float32)
        .astype(jnp.bfloat16)
        .astype(jnp.float32)
    )
    up = jnp.dot(inputs, up_full, preferred_element_type=jnp.float32)
    conv = bias + taps[2] * gate + taps[1] * shift_later(gate, 1) + taps[0] * shift_later(gate, 2)
    act = jax.nn.silu(conv)
    hidden = (act * up).astype(jnp.bfloat16)
    return (conv, act, up, hidden)


def forward_pass(x_late, gate_full, up_full, down_full, taps, bias):
    conv, act, up, hidden = hidden_parts(x_late, gate_full, up_full, taps, bias)
    partial_value = jnp.dot(hidden, down_full, preferred_element_type=jnp.float32)
    return lax.psum(partial_value.astype(jnp.bfloat16), "tp")


def backward_pass(x_early, cotangent, gate_full, up_full, down_full, taps, bias, grad_down):
    conv, act, up, hidden = hidden_parts(x_early, gate_full, up_full, taps, bias)
    dhidden = contract_last(cotangent, down_full)
    summed = lax.psum_scatter(
        lax.dot_general(
            cotangent, hidden, (((0,), (0,)), ((), ())), preferred_element_type=jnp.float32
        ),
        "fs",
        scatter_dimension=0,
        tiled=True,
    )
    grad_down_out = grad_down + summed.T
    dup = (dhidden * act).astype(jnp.bfloat16)
    sig = jax.nn.sigmoid(conv)
    dconv = dhidden * up * sig * (1.0 + conv * (1.0 - sig))
    dgate = taps[2] * dconv + taps[1] * shift_earlier(dconv, 1) + taps[0] * shift_earlier(dconv, 2)
    dgate = dgate.astype(jnp.bfloat16)
    partial_value = contract_last(dup, up_full) + contract_last(dgate, gate_full)
    dx_early = lax.psum(partial_value.astype(jnp.bfloat16), "tp")
    return (dx_early, grad_down_out)


def shards(x_late, x_early, cotangent, w_gate, w_up, w_down, conv_taps, conv_bias, grad_down):
    width = w_gate.shape[1]
    offset = lax.axis_index("tp") * width
    taps = lax.dynamic_slice_in_dim(conv_taps, offset, width, 1)
    bias = lax.dynamic_slice_in_dim(conv_bias, offset, width, 0)
    gate_full, up_full = (
        lax.all_gather(w_gate, "fs", axis=0, tiled=True),
        lax.all_gather(w_up, "fs", axis=0, tiled=True),
    )
    down_full = lax.all_gather(w_down, "fs", axis=1, tiled=True)
    y_late = forward_pass(x_late, gate_full, up_full, down_full, taps, bias)
    dx_early, grad_down_out = backward_pass(
        x_early, cotangent, gate_full, up_full, down_full, taps, bias, grad_down
    )
    return (y_late, dx_early, grad_down_out)


def carry_kernel(pieces, *refs):
    ins, outs, held, r_s, w_s = refs[:3], refs[3:6], refs[6:9], refs[9], refs[10]

    def move(i, p, back):
        rows = ins[i].shape[0] // pieces
        sl = pl.ds(p * rows, rows)
        src, dst = (held[i], outs[i]) if back else (ins[i], held[i])
        return pltpu.make_async_copy(src.at[sl, :], dst.at[sl, :], (w_s if back else r_s).at[i, p])

    steps = [(i, p) for i in range(3) for p in range(pieces)]
    for i, p in steps:
        move(i, p, False).start()
    for i, p in steps:
        move(i, p, False).wait()
        move(i, p, True).start()
    for i, p in steps:
        move(i, p, True).wait()


def carry(*arrays):
    pieces = 2
    return pl.pallas_call(
        functools.partial(carry_kernel, pieces),
        out_shape=tuple(jax.ShapeDtypeStruct(a.shape, a.dtype) for a in arrays),
        in_specs=[ANY] * 3,
        out_specs=(ANY,) * 3,
        scratch_shapes=[pltpu.VMEM(a.shape, a.dtype) for a in arrays]
        + [pltpu.SemaphoreType.DMA((3, pieces))] * 2,
        compiler_params=pltpu.CompilerParams(vmem_limit_bytes=VMEM_BYTES),
        name="results",
    )(*arrays)


def grouped_shards(nz, x_late, x_early, cotangent, w_gate, w_up, w_down, conv_taps, conv_bias, grad_down):
    outputs = layer(
        nz, (x_late, x_early, cotangent), w_gate, w_up, w_down, conv_taps,
        conv_bias.reshape(1, conv_bias.shape[0]), grad_down,
    )
    return carry(*outputs)


def solution(mesh):
    def step(*arrays):
        x_late, w_gate = arrays[0], arrays[3]
        fs, tp = mesh.shape["fs"], mesh.shape["tp"]
        units, rest = divmod(w_gate.shape[1], GROUP)
        lanes_ok = rest == 0 and units % 128 == 0 and w_gate.shape[0] % 128 == 0
        if tp == 2 and fs % GROUP == 0 and lanes_ok and x_late.shape[0] % 32 == 0:
            return grouped_shards(fs // GROUP, *arrays)
        return shards(*arrays)

    placed = (
        P("fs", None),
        P("fs", None),
        P("fs", None),
        P("fs", "tp"),
        P("fs", "tp"),
        P("tp", "fs"),
        P(),
        P(),
        P("tp", "fs"),
    )
    return jax.shard_map(
        step,
        mesh=mesh,
        in_specs=placed,
        out_specs=(P("fs", None), P("fs", None), P("tp", "fs")),
        check_vma=False,
    )
```

```python
import functools

import jax
import jax.numpy as jnp
from jax import lax
from jax.experimental import pallas as pl
from jax.experimental.pallas import tpu as pltpu
from jax.sharding import PartitionSpec as P

GROUP = 4
VMEM_BYTES = 63 * 1024 * 1024
VMEM = pl.BlockSpec(memory_space=pltpu.VMEM)
ANY = pl.BlockSpec(memory_space=pl.ANY)


def place():
    f, c = lax.axis_index("fs"), lax.axis_index("tp")
    q, z = lax.rem(f, GROUP), lax.div(f, GROUP)
    qx = q + 1 - 2 * lax.rem(q, 2)
    qy = q + 2 - 4 * lax.div(q, 2)
    qa, qb = qx + c * (qy - qx), qy + c * (qx - qy)
    return f, c, q, z, qa, qb, GROUP - 1 - q


def at(start, size):
    return pl.ds(pl.multiple_of(start, size), size)


def remote(src, dst, send, recv, **device):
    return pltpu.make_async_remote_copy(
        src_ref=src, dst_ref=dst, send_sem=send, recv_sem=recv,
        device_id=device, device_id_type=pl.DeviceIdType.MESH,
    )


def total(dst, srcs, rows, step=32):
    @pl.loop(0, rows, step=step)
    def _(i):
        sl = pl.ds(pl.multiple_of(i, step), step)
        out = srcs[0][sl, :].astype(jnp.float32)
        for s in srcs[1:]:
            out = out + s[sl, :].astype(jnp.float32)
        dst[sl, :] = out.astype(dst.dtype)


def mm(left, right, dims=((1,), (0,))):
    return lax.dot_general(left, right, (dims, ((), ())), preferred_element_type=jnp.float32)


def layer_kernel(nz, tile, x0, x1, x2, wg, wu, wd, taps, bias, gd_in, y_out, dx_out, g_out,
                 y, dx, g, gd, t0, t1, t2, og, ou, od, hid, hid_t, conv_s, up_s, gate_l, up_l, dup, dgate, yp, xp, gp,
                 core, summed, got, gin_r, gin_l, hand, passed_r, passed_l,
                 loc, w_s, w_r, n_s, n_r, p_s, p_r, r_s, r_r, l_s, l_r,
                 c_s, c_r, a_s, a_r, zr_s, zr_r, zl_s, zl_r, g_s, g_r, pr_s, pr_r, pl_s, pl_r, fr_s, fr_r, fl_s, fl_r, e_s, e_r, o_s):
    f, c, q, z, qa, qb, qd = place()
    base = z * GROUP
    xs, ts, outs = (x0, x1, x2), (t0, t1, t2), (og, ou, od)
    rows, d_model = x0.shape
    half = rows // 2
    r, u = wg.shape[0], og.shape[1]
    wide = GROUP * r
    parts_d = wide // 256 if wide % 256 == 0 else 1
    part, downs = wide // parts_d, range(2, 2 + parts_d)
    first, last = z > 0, z < nz - 1
    low, high = z == 0, z == nz - 1
    units = (c * GROUP + q) * u

    barrier = pltpu.get_barrier_semaphore()
    for peer in (qa, qb, qd):
        pl.semaphore_signal(barrier, 1, device_id={"fs": base + peer}, device_id_type=pl.DeviceIdType.MESH)
    pl.semaphore_signal(barrier, 1, device_id={"tp": 1 - c}, device_id_type=pl.DeviceIdType.MESH)
    @pl.when(last)
    def _():
        pl.semaphore_signal(barrier, 1, device_id={"fs": f + GROUP}, device_id_type=pl.DeviceIdType.MESH)

    @pl.when(first)
    def _():
        pl.semaphore_signal(barrier, 1, device_id={"fs": f - GROUP}, device_id_type=pl.DeviceIdType.MESH)

    beside = lax.div(z + nz - 1, nz) + lax.div(2 * nz - 2 - z, nz)
    pl.semaphore_wait(barrier, GROUP + beside)

    def piece(k, peer):
        if k == 2:
            return wd.at[at(peer * u, u), :]
        return (wg, wu)[k].at[:, at(peer * u, u)]

    def landing(k, owner):
        if k == 2:
            return od.at[:, at(owner * r, r)]
        return outs[k].at[at(owner * r, r), :]

    def block(k, b):
        if k >= 2:
            return od.at[:, at(b * wide + (k - 2) * part, part)]
        return outs[k].at[at(b * wide, wide), :]

    def right(k, s):
        b = block(k, z - s)
        return remote(b, b, r_s.at[s, k], r_r.at[s, k], fs=f + GROUP)

    def left(k, s):
        b = block(k, z + s)
        return remote(b, b, l_s.at[s, k], l_r.at[s, k], fs=f - GROUP)

    def from_left(k, s):
        b = block(k, z - s - 1)
        return remote(b, b, r_s.at[s, k], r_r.at[s, k], fs=f - GROUP)

    def from_right(k, s):
        b = block(k, z + s + 1)
        return remote(b, b, l_s.at[s, k], l_r.at[s, k], fs=f + GROUP)

    def onward(k, s, act):
        @pl.when(jnp.logical_and(z - s >= 0, last))
        def _():
            act(right(k, s))

        @pl.when(jnp.logical_and(z + s < nz, first))
        def _():
            act(left(k, s))

    begin, sent = (lambda copy: copy.start()), (lambda copy: copy.wait_send())

    def along(k, src, owner):
        there = landing(k, owner)

        @pl.when(last)
        def _():
            remote(src, there, r_s.at[0, k], r_r.at[0, k], fs=f + GROUP).start()

        @pl.when(first)
        def _():
            remote(src, there, l_s.at[0, k], l_r.at[0, k], fs=f - GROUP).start()

    def relay(k, s):
        @pl.when(jnp.logical_and(z - s - 1 >= 0, last))
        def _():
            from_left(k, s).wait_recv()
            right(k, s + 1).start()

        @pl.when(jnp.logical_and(z + s + 1 < nz, first))
        def _():
            from_right(k, s).wait_recv()
            left(k, s + 1).start()

    def ended(k, s):
        @pl.when(high)
        def _():
            from_left(k, s).wait_recv()

        @pl.when(low)
        def _():
            from_right(k, s).wait_recv()

    mine, other = at(c * half, half), at((1 - c) * half, half)
    weights, near, local = {}, {}, []

    def spread(k):
        for d, peer in enumerate((qa, qb, qd)):
            copy = remote(piece(k, peer), landing(k, f), w_s.at[k, d], w_r.at[k, d], fs=base + peer)
            copy.start()
            weights[k, d] = copy

    def share(i):
        for d, peer in enumerate((qa, qb)):
            copy = remote(xs[i].at[mine, :], ts[i].at[q, mine, :], n_s.at[i, d], n_r.at[i, d], fs=base + peer)
            copy.start()
            near[i, d] = copy

    along(0, piece(0, q), f)
    spread(0)
    along(1, piece(1, q), f)
    spread(1)
    share(1)
    share(0)
    spread(2)
    share(2)
    for k in range(3):
        copy = pltpu.make_async_copy(piece(k, q), landing(k, f), loc.at[k])
        copy.start()
        local.append(copy)
    for i in range(3):
        copy = pltpu.make_async_copy(xs[i], ts[i].at[q], loc.at[3 + i])
        copy.start()
        local.append(copy)

    old_grad = pltpu.make_async_copy(gd_in, gd, loc.at[6])
    old_grad.start()

    row = lax.broadcasted_iota(jnp.int32, (rows, tile), 0)

    def later(v, steps):
        return jnp.where(row >= steps, pltpu.roll(v, steps, 0), 0.0)

    def earlier(v, steps):
        return jnp.where(row < rows - steps, pltpu.roll(v, rows - steps, 0), 0.0)

    upper = lax.div(2 * z, nz)
    head_k = pl.ds(pl.multiple_of(upper * wide, wide), max(nz - 1, 1) * wide)
    tail_k = at((1 - upper) * (nz - 1) * wide, wide)

    def begun(i):
        t, kept_gate, kept_up = ((t0, gate_l, up_l), (t1, conv_s, up_s))[i]

        @pl.loop(0, GROUP)
        def _(b):
            @pl.loop(0, u // tile)
            def _(j):
                cols, seq = at(j * tile, tile), at(b * rows, rows)
                x = t[b, :, head_k]
                kept_gate[seq, cols] = mm(x, og[head_k, cols])
                kept_up[seq, cols] = mm(x, ou[head_k, cols])

    def forward(i, split):
        t, kept_gate, kept_up = ((t0, gate_l, up_l), (t1, conv_s, up_s))[i]
        keep = i == 1

        @pl.loop(0, GROUP)
        def _(b):
            @pl.loop(0, u // tile)
            def _(j):
                cols, seq, par = at(j * tile, tile), at(b * rows, rows), at(units + j * tile, tile)
                if split:
                    x = t[b, :, tail_k]
                    gate = kept_gate[seq, cols] + mm(x, og[tail_k, cols])
                    up = kept_up[seq, cols] + mm(x, ou[tail_k, cols])
                else:
                    x = t[b]
                    gate, up = mm(x, og[:, cols]), mm(x, ou[:, cols])
                gate = gate.astype(jnp.bfloat16).astype(jnp.float32)
                conv = (bias[:, par] + taps[2:3, par] * gate + taps[1:2, par] * later(gate, 1)
                        + taps[0:1, par] * later(gate, 2))
                out = conv / (1.0 + jnp.exp(-conv)) * up
                if keep:
                    conv_s[seq, cols] = conv
                    up_s[seq, cols] = up
                    hid_t[at(j * tile, tile), seq] = out.T.astype(jnp.bfloat16)
                else:
                    hid[seq, cols] = out.astype(jnp.bfloat16)

    def to_owners(o, into, send_sems, recv_sems, act):
        for d, peer in enumerate((qa, qb, qd)):
            src = gp.at[:, at(o * wide + peer * r, r)]
            act(remote(src, into.at[at(q * u, u), :], send_sems.at[d], recv_sems.at[d], fs=base + peer))

    def keep_own(o, into):
        into[at(q * u, u), :] = gp[:, at(o * wide + q * r, r)]

    def exchange(act):
        to_owners(z, hand, g_s, g_r, act)

    def passing_r(act):
        to_owners(nz - 1, passed_r, pr_s, pr_r, act)

    def passing_l(act):
        to_owners(0, passed_l, pl_s, pl_r, act)

    def passed_on_r():
        return remote(passed_r, passed_r, fr_s.at[0], fr_r.at[0], fs=f + GROUP)

    def passed_on_l():
        return remote(passed_l, passed_l, fl_s.at[0], fl_r.at[0], fs=f - GROUP)

    arrival = lambda copy: copy.wait_recv()

    def hand_on():
        @pl.when(z == nz - 2)
        def _():
            passing_r(arrival)
            passed_on_r().start()

        @pl.when(z == 1)
        def _():
            passing_l(arrival)
            passed_on_l().start()

    def slot_r(o, m, e):
        there = gin_r.at[m, :, pl.ds(e * part, part)]
        return remote(gp.at[:, at(o * wide + e * part, part)], there, zr_s.at[m, e], zr_r.at[m, e], fs=f + GROUP)

    def slot_l(o, m, e):
        there = gin_l.at[m, :, pl.ds(e * part, part)]
        return remote(gp.at[:, at(o * wide + e * part, part)], there, zl_s.at[m, e], zl_r.at[m, e], fs=f - GROUP)

    halves = range(parts_d)

    def pass_part(o, into, send_sems, recv_sems, e):
        for d, peer in enumerate((qa, qb, qd)):
            @pl.when(lax.div(peer * r, part) == e)
            def _(d=d, peer=peer):
                src = gp.at[:, at(o * wide + peer * r, r)]
                remote(src, into.at[at(q * u, u), :], send_sems.at[d], recv_sems.at[d], fs=base + peer).start()
        if e == parts_d - 1:
            keep_own(o, into)

    def rightward(o, m, e):
        if m < nz - 2:
            slot_r(o, m, e).start()
            return

        @pl.when(z == nz - 2)
        def _():
            pass_part(nz - 1, passed_r, pr_s, pr_r, e)

        @pl.when(z < nz - 2)
        def _():
            slot_r(o, m, e).start()

    def leftward(o, m, e):
        if m < nz - 2:
            slot_l(o, m, e).start()
            return

        @pl.when(z == 1)
        def _():
            pass_part(0, passed_l, pl_s, pl_r, e)

        @pl.when(z > 1)
        def _():
            slot_l(o, m, e).start()

    def down_grad():
        for i in range(nz):
            o = nz - 1 - i + upper * (2 * i - (nz - 1))
            cols = at(o * wide, wide)
            cot = t2[:, :, cols].reshape(GROUP * rows, wide)
            gp[:, cols] = mm(hid_t[...], cot).astype(jnp.bfloat16)
            if i < nz - 1:
                @pl.when(low)
                def _():
                    for e in halves:
                        rightward(o, i, e)

                @pl.when(high)
                def _():
                    for e in halves:
                        leftward(o, i, e)

        @pl.when(jnp.logical_or(low, high))
        def _():
            exchange(begin)

    def settle():
        @pl.when(jnp.logical_and(first, last))
        def _():
            m = nz - 2
            for e in halves:
                slot_r(z, m, e).wait_recv()
                slot_l(z, m, e).wait_recv()
            home = gp.at[:, at(z * wide, wide)]
            total(home, [home, gin_r.at[m], gin_l.at[m]], u)
            exchange(begin)

    def chain(j, e):
        o, p = nz - 2 + z - j, z + 2 - nz + j
        here = pl.ds(e * part, part)

        @pl.when(jnp.logical_and(first, o <= nz - 1))
        def _():
            slot_r(o, j, e).wait_recv()
            cols = at(o * wide + e * part, part)
            total(gp.at[:, cols], [gp.at[:, cols], gin_r.at[j, :, here]], u)
            rightward(o, j + 1, e)

        @pl.when(jnp.logical_and(last, p >= 0))
        def _():
            slot_l(p, j, e).wait_recv()
            cols = at(p * wide + e * part, part)
            total(gp.at[:, cols], [gp.at[:, cols], gin_l.at[j, :, here]], u)
            leftward(p, j + 1, e)

    def backward(n):
        b, out = order[n], pl.ds(n * rows, rows)

        @pl.loop(0, u // tile)
        def _(j):
            cols, seq, par = at(j * tile, tile), at(b * rows, rows), at(units + j * tile, tile)
            dh = mm(t2[b], od[at(j * tile, tile), :], ((1,), (1,)))
            conv = conv_s[seq, cols]
            sig = 1.0 / (1.0 + jnp.exp(-conv))
            dup[out, cols] = (dh * (conv * sig)).astype(jnp.bfloat16)
            dc = dh * up_s[seq, cols] * sig * (1.0 + conv * (1.0 - sig))
            dg = (taps[2:3, par] * dc + taps[1:2, par] * earlier(dc, 1)
                  + taps[0:1, par] * earlier(dc, 2))
            dgate[out, cols] = dg.astype(jnp.bfloat16)

    mirrored = z + upper * (nz - 1 - 2 * z)

    def turn(i):
        near_side = lax.div(mirrored - i + nz, nz)
        v = i + near_side * (mirrored - 2 * i)
        return v + upper * (nz - 1 - 2 * v)


    def late_start(h):
        return turn(h // parts_d) * wide + h % parts_d * part if isinstance(h, int) else (
            turn(lax.div(h, parts_d)) * wide + lax.rem(h, parts_d) * part)

    def late_block(h):
        cols = at(late_start(h), part)
        yp[:, cols] = mm(hid[...], od[:, cols]).astype(jnp.bfloat16)

    parts, finals, results = (yp, xp), (y, dx), (y_out, dx_out)
    order = (qd, qa, qb, q)
    theirs = (qd, qb, qa, q)
    places = ((order, theirs), ((0, 1, 2, 3), (0, 2, 1, 3)))

    def span(t, i):
        return at(late_start(i), part) if t == 0 else at(i * wide, wide)

    def core_copy(t, i, n):
        cols = span(t, i)
        src = parts[t].at[at(places[t][1][n] * rows + (1 - c) * half, half), cols]
        return remote(src, core.at[t, n, :, cols], c_s.at[t, i, n], c_r.at[t, i, n], tp=1 - c)

    def to_core(t, i):
        for n in range(4):
            core_copy(t, i, n).start()

    def plane_copy(t, i, slot):
        cols = span(t, i)
        src = core.at[t, 0, :, cols] if slot == 2 else summed.at[t, slot, :, cols]
        return remote(src, got.at[t, slot, :, cols], a_s.at[t, i, slot], a_r.at[t, i, slot],
                      fs=base + (qb if slot == 2 else qa))

    def join_one(t, i, n):
        cols = span(t, i)
        core_copy(t, i, n).wait_recv()
        own = parts[t].at[at(places[t][0][n] * rows + c * half, half), cols]
        total(summed.at[t, n, :, cols], [own, core.at[t, n, :, cols]], half)
        if n < 2:
            plane_copy(t, i, n).start()

    def join(t, i):
        for n in range(4):
            join_one(t, i, n)

    def second(t, i):
        cols = span(t, i)
        plane_copy(t, i, 0).wait_recv()
        total(core.at[t, 0, :, cols], [summed.at[t, 2, :, cols], got.at[t, 0, :, cols]], half)
        plane_copy(t, i, 2).start()

    def end_copy(t, i):
        cols = span(t, i)
        return remote(finals[t].at[:, cols], results[t].at[mine, cols], e_s.at[t, i], e_r.at[t, i], tp=1 - c)

    def own_copy(t, i):
        cols = span(t, i)
        return pltpu.make_async_copy(finals[t].at[:, cols], results[t].at[mine, cols], o_s.at[t, i])

    def finish(t, i):
        cols = span(t, i)
        plane_copy(t, i, 1).wait_recv()
        plane_copy(t, i, 2).wait_recv()
        total(finals[t].at[:, cols], [summed.at[t, 3, :, cols], got.at[t, 1, :, cols], got.at[t, 2, :, cols]], half)
        end_copy(t, i).start()
        own_copy(t, i).start()

    blocks = (nz * parts_d, nz)

    def each(fn, t=1):
        @pl.loop(0, blocks[t])
        def _(i):
            fn(i)

    def early_piece(n, m, i):
        seq, cols = pl.ds(n * rows, m * rows), at(i * wide, wide)
        out = mm(dup[seq, :], ou[cols, :], ((1,), (1,))) + mm(dgate[seq, :], og[cols, :], ((1,), (1,)))
        xp[seq, cols] = out.astype(jnp.bfloat16)
        for k in range(n, n + m):
            core_copy(1, i, (0, 2, 1, 3)[k]).start()

    def first_out():
        for i in range(nz + 2):
            if i < nz:
                early_piece(0, 1, i)
            if i > 1:
                join_one(1, i - 2, 0)

    def pair_out():
        for i in range(nz + 1):
            if i < nz:
                early_piece(1, 2, i)
            if i > 0:
                join_one(1, i - 1, 2)
                join_one(1, i - 1, 1)
            if 1 < i < nz:
                second(1, i - 2)

    def last_out():
        each(lambda i: early_piece(3, 1, i))

    def joins(n):
        each(lambda i: join_one(1, i, n))

    def finishes(t):
        each(lambda i: finish(t, i), t)

    def ended_out(t):
        each(lambda i: end_copy(t, i).wait_recv(), t)

    partner, far = [], {}

    def pass_on(i, owner, kind):
        there = ts[i].at[owner, mine, :]
        copy = remote(there, there, p_s.at[i, kind], p_r.at[i, kind], tp=1 - c)
        copy.start()
        partner.append(copy)

    def adjacent(i):
        near[i, 0].wait_recv()
        there = ts[i].at[qa, mine, :]
        copy = remote(there, there, n_s.at[i, 2], n_r.at[i, 2], fs=base + qb)
        copy.start()
        far[i] = copy
        pass_on(i, qa, 0)
        near[i, 1].wait_recv()
        pass_on(i, qb, 1)

    def opposite(i):
        far[i].wait_recv()
        pass_on(i, qd, 2)

    def complete(i):
        for kind, owner in enumerate((qb, qa, qd)):
            there = ts[i].at[owner, other, :]
            remote(there, there, p_s.at[i, kind], p_r.at[i, kind], tp=1 - c).wait_recv()
        local[3 + i].wait()

    for k in range(2):
        for d, peer in enumerate((qa, qb, qd)):
            weights[k, d].wait_recv()
            along(k, landing(k, base + peer), base + peer)
        local[k].wait()
    adjacent(1)
    if nz > 2:
        relay(0, 0)
        relay(1, 0)
    adjacent(0)
    for d in range(3):
        weights[2, d].wait_recv()
    local[2].wait()
    for s in range(1, nz - 2):
        relay(0, s)
        relay(1, s)
    for k in downs:
        onward(k, 0, begin)
    adjacent(2)
    at_end = jnp.logical_or(low, high) if nz > 1 else z < 0
    inside = jnp.logical_and(first, last) if nz > 1 else z >= 0

    def forward_head(i):
        @pl.when(at_end)
        def _():
            begun(i)

        @pl.when(inside)
        def _():
            forward(i, False)

    def forward_tail(i):
        @pl.when(at_end)
        def _():
            forward(i, True)

    opposite(1)
    complete(1)
    for s in range(nz - 2):
        ended(0, s)
        ended(1, s)
    if nz > 2:
        for k in downs:
            relay(k, 0)
    forward_head(1)
    opposite(0)
    complete(0)
    forward_head(0)
    for s in range(1, nz - 2):
        for k in downs:
            relay(k, s)
    if nz > 1:
        ended(0, nz - 2)
        ended(1, nz - 2)
    forward_tail(1)
    opposite(2)
    complete(2)
    down_grad()
    forward_tail(0)

    count = blocks[0]

    @pl.when(at_end)
    def _():
        progress = [0, 0]

        def catch_up(stage, upto):
            while progress[stage] <= upto:
                (join, second)[stage](0, progress[stage])
                progress[stage] += 1

        for h in range(count - 1):
            i, p = divmod(h, parts_d)
            if i > 0:
                ended(2 + p, i - 1)
            late_block(h)
            to_core(0, h)
            if h > 2:
                catch_up(1, h - 3)
            catch_up(0, h - 1)
            if h in (parts_d * (nz - 2) - 1, parts_d * (nz - 1) - 1):
                catch_up(0, h)
                catch_up(1, h - 1)
        catch_up(0, count - 2)
        catch_up(1, count - 3)
        if nz > 1:
            ended(1 + parts_d, nz - 2)
        late_block(count - 1)
        to_core(0, count - 1)

    @pl.when(inside)
    def _():
        for h in range(count):
            late_block(h)
            to_core(0, h)
            if h > 1:
                join(0, h - 2)
        for h in range(max(count - 2, 0), count - 1):
            join(0, h)

    def seconds_late(begin_at):
        @pl.loop(begin_at, count)
        def _(h):
            second(0, h)

    if nz > 2:
        chain(0, 0)
    def grad_sum(*extra):
        @pl.loop(0, GROUP * u, step=128)
        def _(i):
            sl = at(i, 128)
            out = hand[sl, :].astype(jnp.float32)
            for e in extra:
                out = out + e[sl, :].astype(jnp.float32)
            g[sl, :] = gd[sl, :] + out

    g_copy = pltpu.make_async_copy(g, g_out, loc.at[8])

    def grad_out():
        exchange(arrival)
        keep_own(z, hand)
        old_grad.wait()

        @pl.when(inside)
        def _():
            grad_sum()

        if nz > 1:
            @pl.when(high)
            def _():
                passed_on_r().wait_recv()
                grad_sum(passed_r)

            @pl.when(low)
            def _():
                passed_on_l().wait_recv()
                grad_sum(passed_l)

        g_copy.start()

    backward(0)
    join(0, count - 1)
    first_out()
    for e in range(1, parts_d if nz > 2 else 0):
        chain(0, e)

    @pl.when(at_end)
    def _():
        seconds_late(max(count - 2, 0))

    @pl.when(inside)
    def _():
        seconds_late(0)

    backward(1)
    backward(2)
    for j in range(1, nz - 2):
        for e in halves:
            chain(j, e)
    pair_out()
    if nz > 1:
        hand_on()
    for i in range(max(nz - 2, 0), nz):
        second(1, i)
    backward(3)
    if nz > 1:
        settle()
    last_out()
    joins(3)
    finishes(0)

    @pl.when(at_end)
    def _():
        for i in range(nz - 1):
            finish(1, i)
        grad_out()
        finish(1, nz - 1)

    @pl.when(inside)
    def _():
        finishes(1)
        grad_out()

    for t in range(2):
        ended_out(t)
    for copies in (weights, near, far):
        for copy in copies.values():
            copy.wait_send()
    for copy in partner:
        copy.wait_send()
    exchange(sent)
    for t in range(2):
        @pl.loop(0, blocks[t])
        def _(i, t=t):
            for n in range(4):
                core_copy(t, i, n).wait_send()
            for slot in range(3):
                plane_copy(t, i, slot).wait_send()
            end_copy(t, i).wait_send()
            own_copy(t, i).wait()
    for s in range(nz - 1):
        for k in range(2 + parts_d):
            onward(k, s, sent)
    for m in range(nz - 2):
        @pl.when(jnp.logical_and(last, z <= m))
        def _(m=m):
            for e in halves:
                slot_r(0, m, e).wait_send()

        @pl.when(jnp.logical_and(first, nz - 1 - z <= m))
        def _(m=m):
            for e in halves:
                slot_l(0, m, e).wait_send()

    if nz > 1:
        @pl.when(z < nz - 2)
        def _():
            for e in halves:
                slot_r(0, nz - 2, e).wait_send()

        @pl.when(z == nz - 2)
        def _():
            passing_r(sent)
            passed_on_r().wait_send()

        @pl.when(z > 1)
        def _():
            for e in halves:
                slot_l(0, nz - 2, e).wait_send()

        @pl.when(z == 1)
        def _():
            passing_l(sent)
            passed_on_l().wait_send()

    g_copy.wait()


def layer(nz, xs, w_gate, w_up, w_down, taps, bias, grad_down):
    rows, d = xs[0].shape
    u = w_gate.shape[1] // GROUP
    r = w_gate.shape[0]
    half, toks, wide = rows // 2, GROUP * rows, GROUP * r
    tile = 256 if u % 256 == 0 else 128
    sems = lambda *shape: [pltpu.SemaphoreType.DMA(shape)] * 2
    b16, f32 = jnp.bfloat16, jnp.float32
    out = jax.ShapeDtypeStruct((rows, d), b16)
    hops = max(nz - 1, 1)
    parts_d = wide // 256 if wide % 256 == 0 else 1
    count = nz * parts_d
    return pl.pallas_call(
        functools.partial(layer_kernel, nz, tile),
        out_shape=(out, out, jax.ShapeDtypeStruct((u * GROUP, r), f32)),
        in_specs=[ANY] * 6 + [VMEM] * 2 + [ANY],
        out_specs=(ANY,) * 3,
        scratch_shapes=[pltpu.VMEM((half, d), b16)] * 2
        + [pltpu.VMEM((u * GROUP, r), f32)] * 2
        + [pltpu.VMEM((GROUP, rows, d), b16)] * 3
        + [pltpu.VMEM((d, u), b16)] * 2
        + [pltpu.VMEM((u, d), b16), pltpu.VMEM((toks, u), b16), pltpu.VMEM((u, toks), b16),
           pltpu.VMEM((toks, u), f32), pltpu.VMEM((toks, u), f32),
           pltpu.VMEM((toks, u), f32), pltpu.VMEM((toks, u), f32),
           pltpu.VMEM((toks, u), b16), pltpu.VMEM((toks, u), b16),
           pltpu.VMEM((toks, d), b16), pltpu.VMEM((toks, d), b16), pltpu.VMEM((u, d), b16),
           pltpu.VMEM((2, 4, half, d), b16), pltpu.VMEM((2, 4, half, d), b16), pltpu.VMEM((2, 3, half, d), b16),
           pltpu.VMEM((hops, u, wide), b16), pltpu.VMEM((hops, u, wide), b16)]
        + [pltpu.VMEM((u * GROUP, r), b16)] * 3
        + [pltpu.SemaphoreType.DMA((10,))]
        + sems(3, 3) + sems(3, 3) + sems(3, 3) + sems(hops, 2 + parts_d) + sems(hops, 2 + parts_d)
        + sems(2, count, 4) + sems(2, count, 3) + sems(hops, parts_d) + sems(hops, parts_d) + sems(3)
        + sems(3) + sems(3) + sems(1) + sems(1) + sems(2, count)
        + [pltpu.SemaphoreType.DMA((2, count))],
        compiler_params=pltpu.CompilerParams(collective_id=0, has_side_effects=True, vmem_limit_bytes=VMEM_BYTES),
        name="layer_group",
    )(*xs, w_gate, w_up, w_down, taps, bias, grad_down)


def shift_later(field, steps):
    pad = jnp.zeros((steps, field.shape[1]), jnp.float32)
    return jnp.concatenate([pad, field[: field.shape[0] - steps]], axis=0)


def shift_earlier(field, steps):
    pad = jnp.zeros((steps, field.shape[1]), jnp.float32)
    return jnp.concatenate([field[steps:], pad], axis=0)


def contract_last(left, right):
    return lax.dot_general(
        left, right, (((1,), (1,)), ((), ())), preferred_element_type=jnp.float32
    )


def hidden_parts(inputs, gate_full, up_full, taps, bias):
    gate = (
        jnp.dot(inputs, gate_full, preferred_element_type=jnp.float32)
        .astype(jnp.bfloat16)
        .astype(jnp.float32)
    )
    up = jnp.dot(inputs, up_full, preferred_element_type=jnp.float32)
    conv = bias + taps[2] * gate + taps[1] * shift_later(gate, 1) + taps[0] * shift_later(gate, 2)
    act = jax.nn.silu(conv)
    hidden = (act * up).astype(jnp.bfloat16)
    return (conv, act, up, hidden)


def forward_pass(x_late, gate_full, up_full, down_full, taps, bias):
    conv, act, up, hidden = hidden_parts(x_late, gate_full, up_full, taps, bias)
    partial_value = jnp.dot(hidden, down_full, preferred_element_type=jnp.float32)
    return lax.psum(partial_value.astype(jnp.bfloat16), "tp")


def backward_pass(x_early, cotangent, gate_full, up_full, down_full, taps, bias, grad_down):
    conv, act, up, hidden = hidden_parts(x_early, gate_full, up_full, taps, bias)
    dhidden = contract_last(cotangent, down_full)
    summed = lax.psum_scatter(
        lax.dot_general(
            cotangent, hidden, (((0,), (0,)), ((), ())), preferred_element_type=jnp.float32
        ),
        "fs",
        scatter_dimension=0,
        tiled=True,
    )
    grad_down_out = grad_down + summed.T
    dup = (dhidden * act).astype(jnp.bfloat16)
    sig = jax.nn.sigmoid(conv)
    dconv = dhidden * up * sig * (1.0 + conv * (1.0 - sig))
    dgate = taps[2] * dconv + taps[1] * shift_earlier(dconv, 1) + taps[0] * shift_earlier(dconv, 2)
    dgate = dgate.astype(jnp.bfloat16)
    partial_value = contract_last(dup, up_full) + contract_last(dgate, gate_full)
    dx_early = lax.psum(partial_value.astype(jnp.bfloat16), "tp")
    return (dx_early, grad_down_out)


def shards(x_late, x_early, cotangent, w_gate, w_up, w_down, conv_taps, conv_bias, grad_down):
    width = w_gate.shape[1]
    offset = lax.axis_index("tp") * width
    taps = lax.dynamic_slice_in_dim(conv_taps, offset, width, 1)
    bias = lax.dynamic_slice_in_dim(conv_bias, offset, width, 0)
    gate_full, up_full = (
        lax.all_gather(w_gate, "fs", axis=0, tiled=True),
        lax.all_gather(w_up, "fs", axis=0, tiled=True),
    )
    down_full = lax.all_gather(w_down, "fs", axis=1, tiled=True)
    y_late = forward_pass(x_late, gate_full, up_full, down_full, taps, bias)
    dx_early, grad_down_out = backward_pass(
        x_early, cotangent, gate_full, up_full, down_full, taps, bias, grad_down
    )
    return (y_late, dx_early, grad_down_out)


def carry_kernel(pieces, *refs):
    ins, outs, held, r_s, w_s = refs[:3], refs[3:6], refs[6:9], refs[9], refs[10]

    def move(i, p, back):
        rows = ins[i].shape[0] // pieces
        sl = pl.ds(p * rows, rows)
        src, dst = (held[i], outs[i]) if back else (ins[i], held[i])
        return pltpu.make_async_copy(src.at[sl, :], dst.at[sl, :], (w_s if back else r_s).at[i, p])

    steps = [(i, p) for i in range(3) for p in range(pieces)]
    for i, p in steps:
        move(i, p, False).start()
    for i, p in steps:
        move(i, p, False).wait()
        move(i, p, True).start()
    for i, p in steps:
        move(i, p, True).wait()


def carry(*arrays):
    pieces = 2
    return pl.pallas_call(
        functools.partial(carry_kernel, pieces),
        out_shape=tuple(jax.ShapeDtypeStruct(a.shape, a.dtype) for a in arrays),
        in_specs=[ANY] * 3,
        out_specs=(ANY,) * 3,
        scratch_shapes=[pltpu.VMEM(a.shape, a.dtype) for a in arrays]
        + [pltpu.SemaphoreType.DMA((3, pieces))] * 2,
        compiler_params=pltpu.CompilerParams(vmem_limit_bytes=VMEM_BYTES),
        name="results",
    )(*arrays)


def grouped_shards(nz, x_late, x_early, cotangent, w_gate, w_up, w_down, conv_taps, conv_bias, grad_down):
    outputs = layer(
        nz, (x_late, x_early, cotangent), w_gate, w_up, w_down, conv_taps,
        conv_bias.reshape(1, conv_bias.shape[0]), grad_down,
    )
    return carry(*outputs)


def solution(mesh):
    def step(*arrays):
        x_late, w_gate = arrays[0], arrays[3]
        fs, tp = mesh.shape["fs"], mesh.shape["tp"]
        units, rest = divmod(w_gate.shape[1], GROUP)
        lanes_ok = rest == 0 and units % 128 == 0 and w_gate.shape[0] % 128 == 0
        if tp == 2 and fs % GROUP == 0 and lanes_ok and x_late.shape[0] % 32 == 0:
            return grouped_shards(fs // GROUP, *arrays)
        return shards(*arrays)

    placed = (
        P("fs", None),
        P("fs", None),
        P("fs", None),
        P("fs", "tp"),
        P("fs", "tp"),
        P("tp", "fs"),
        P(),
        P(),
        P("tp", "fs"),
    )
    return jax.shard_map(
        step,
        mesh=mesh,
        in_specs=placed,
        out_specs=(P("fs", None), P("fs", None), P("tp", "fs")),
        check_vma=False,
    )
```

```python
import functools

import jax
import jax.numpy as jnp
from jax import lax
from jax.experimental import pallas as pl
from jax.experimental.pallas import tpu as pltpu
from jax.sharding import PartitionSpec as P

GROUP = 4
VMEM_BYTES = 63 * 1024 * 1024
VMEM = pl.BlockSpec(memory_space=pltpu.VMEM)
ANY = pl.BlockSpec(memory_space=pl.ANY)


def place():
    f, c = lax.axis_index("fs"), lax.axis_index("tp")
    q, z = lax.rem(f, GROUP), lax.div(f, GROUP)
    qx = q + 1 - 2 * lax.rem(q, 2)
    qy = q + 2 - 4 * lax.div(q, 2)
    qa, qb = qx + c * (qy - qx), qy + c * (qx - qy)
    return f, c, q, z, qa, qb, GROUP - 1 - q


def at(start, size):
    return pl.ds(pl.multiple_of(start, size), size)


def remote(src, dst, send, recv, **device):
    return pltpu.make_async_remote_copy(
        src_ref=src, dst_ref=dst, send_sem=send, recv_sem=recv,
        device_id=device, device_id_type=pl.DeviceIdType.MESH,
    )


def total(dst, srcs, rows, step=32):
    @pl.loop(0, rows, step=step)
    def _(i):
        sl = pl.ds(pl.multiple_of(i, step), step)
        out = srcs[0][sl, :].astype(jnp.float32)
        for s in srcs[1:]:
            out = out + s[sl, :].astype(jnp.float32)
        dst[sl, :] = out.astype(dst.dtype)


def mm(left, right, dims=((1,), (0,))):
    return lax.dot_general(left, right, (dims, ((), ())), preferred_element_type=jnp.float32)


def layer_kernel(nz, tile, x0, x1, x2, wg, wu, wd, taps, bias, gd_in, y_out, dx_out, g_out,
                 y, dx, g, gd, t0, t1, t2, og, ou, od, hid, hid_t, conv_s, up_s, gate_l, up_l, dup, dgate, yp, xp, gp,
                 core, summed, got, gin_r, gin_l, hand, passed_r, passed_l,
                 loc, w_s, w_r, n_s, n_r, p_s, p_r, r_s, r_r, l_s, l_r,
                 c_s, c_r, a_s, a_r, zr_s, zr_r, zl_s, zl_r, g_s, g_r, pr_s, pr_r, pl_s, pl_r, fr_s, fr_r, fl_s, fl_r, e_s, e_r, o_s):
    f, c, q, z, qa, qb, qd = place()
    base = z * GROUP
    xs, ts, outs = (x0, x1, x2), (t0, t1, t2), (og, ou, od)
    rows, d_model = x0.shape
    half = rows // 2
    r, u = wg.shape[0], og.shape[1]
    wide = GROUP * r
    parts_d = wide // 256 if wide % 256 == 0 else 1
    part, downs = wide // parts_d, range(2, 2 + parts_d)
    first, last = z > 0, z < nz - 1
    low, high = z == 0, z == nz - 1
    units = (c * GROUP + q) * u

    barrier = pltpu.get_barrier_semaphore()
    for peer in (qa, qb, qd):
        pl.semaphore_signal(barrier, 1, device_id={"fs": base + peer}, device_id_type=pl.DeviceIdType.MESH)
    pl.semaphore_signal(barrier, 1, device_id={"tp": 1 - c}, device_id_type=pl.DeviceIdType.MESH)
    @pl.when(last)
    def _():
        pl.semaphore_signal(barrier, 1, device_id={"fs": f + GROUP}, device_id_type=pl.DeviceIdType.MESH)

    @pl.when(first)
    def _():
        pl.semaphore_signal(barrier, 1, device_id={"fs": f - GROUP}, device_id_type=pl.DeviceIdType.MESH)

    beside = lax.div(z + nz - 1, nz) + lax.div(2 * nz - 2 - z, nz)
    pl.semaphore_wait(barrier, GROUP + beside)

    def piece(k, peer):
        if k == 2:
            return wd.at[at(peer * u, u), :]
        return (wg, wu)[k].at[:, at(peer * u, u)]

    def landing(k, owner):
        if k == 2:
            return od.at[:, at(owner * r, r)]
        return outs[k].at[at(owner * r, r), :]

    def block(k, b):
        if k >= 2:
            return od.at[:, at(b * wide + (k - 2) * part, part)]
        return outs[k].at[at(b * wide, wide), :]

    def right(k, s):
        b = block(k, z - s)
        return remote(b, b, r_s.at[s, k], r_r.at[s, k], fs=f + GROUP)

    def left(k, s):
        b = block(k, z + s)
        return remote(b, b, l_s.at[s, k], l_r.at[s, k], fs=f - GROUP)

    def from_left(k, s):
        b = block(k, z - s - 1)
        return remote(b, b, r_s.at[s, k], r_r.at[s, k], fs=f - GROUP)

    def from_right(k, s):
        b = block(k, z + s + 1)
        return remote(b, b, l_s.at[s, k], l_r.at[s, k], fs=f + GROUP)

    def onward(k, s, act):
        @pl.when(jnp.logical_and(z - s >= 0, last))
        def _():
            act(right(k, s))

        @pl.when(jnp.logical_and(z + s < nz, first))
        def _():
            act(left(k, s))

    begin, sent = (lambda copy: copy.start()), (lambda copy: copy.wait_send())

    def along(k, src, owner):
        there = landing(k, owner)

        @pl.when(last)
        def _():
            remote(src, there, r_s.at[0, k], r_r.at[0, k], fs=f + GROUP).start()

        @pl.when(first)
        def _():
            remote(src, there, l_s.at[0, k], l_r.at[0, k], fs=f - GROUP).start()

    def relay(k, s):
        @pl.when(jnp.logical_and(z - s - 1 >= 0, last))
        def _():
            from_left(k, s).wait_recv()
            right(k, s + 1).start()

        @pl.when(jnp.logical_and(z + s + 1 < nz, first))
        def _():
            from_right(k, s).wait_recv()
            left(k, s + 1).start()

    def ended(k, s):
        @pl.when(high)
        def _():
            from_left(k, s).wait_recv()

        @pl.when(low)
        def _():
            from_right(k, s).wait_recv()

    mine, other = at(c * half, half), at((1 - c) * half, half)
    weights, near, local = {}, {}, []

    def spread(k):
        for d, peer in enumerate((qa, qb, qd)):
            copy = remote(piece(k, peer), landing(k, f), w_s.at[k, d], w_r.at[k, d], fs=base + peer)
            copy.start()
            weights[k, d] = copy

    def share(i):
        for d, peer in enumerate((qa, qb)):
            copy = remote(xs[i].at[mine, :], ts[i].at[q, mine, :], n_s.at[i, d], n_r.at[i, d], fs=base + peer)
            copy.start()
            near[i, d] = copy

    along(0, piece(0, q), f)
    spread(0)
    along(1, piece(1, q), f)
    spread(1)
    share(1)
    share(0)
    spread(2)
    share(2)
    for k in range(3):
        copy = pltpu.make_async_copy(piece(k, q), landing(k, f), loc.at[k])
        copy.start()
        local.append(copy)
    for i in range(3):
        copy = pltpu.make_async_copy(xs[i], ts[i].at[q], loc.at[3 + i])
        copy.start()
        local.append(copy)

    old_grad = pltpu.make_async_copy(gd_in, gd, loc.at[6])
    old_grad.start()

    row = lax.broadcasted_iota(jnp.int32, (rows, tile), 0)

    def later(v, steps):
        return jnp.where(row >= steps, pltpu.roll(v, steps, 0), 0.0)

    def earlier(v, steps):
        return jnp.where(row < rows - steps, pltpu.roll(v, rows - steps, 0), 0.0)

    upper = lax.div(2 * z, nz)
    head_k = pl.ds(pl.multiple_of(upper * wide, wide), max(nz - 1, 1) * wide)
    tail_k = at((1 - upper) * (nz - 1) * wide, wide)

    def begun(i):
        t, kept_gate, kept_up = ((t0, gate_l, up_l), (t1, conv_s, up_s))[i]

        @pl.loop(0, GROUP)
        def _(b):
            @pl.loop(0, u // tile)
            def _(j):
                cols, seq = at(j * tile, tile), at(b * rows, rows)
                x = t[b, :, head_k]
                kept_gate[seq, cols] = mm(x, og[head_k, cols])
                kept_up[seq, cols] = mm(x, ou[head_k, cols])

    def forward(i, split):
        t, kept_gate, kept_up = ((t0, gate_l, up_l), (t1, conv_s, up_s))[i]
        keep = i == 1

        @pl.loop(0, GROUP)
        def _(b):
            @pl.loop(0, u // tile)
            def _(j):
                cols, seq, par = at(j * tile, tile), at(b * rows, rows), at(units + j * tile, tile)
                if split:
                    x = t[b, :, tail_k]
                    gate = kept_gate[seq, cols] + mm(x, og[tail_k, cols])
                    up = kept_up[seq, cols] + mm(x, ou[tail_k, cols])
                else:
                    x = t[b]
                    gate, up = mm(x, og[:, cols]), mm(x, ou[:, cols])
                gate = gate.astype(jnp.bfloat16).astype(jnp.float32)
                conv = (bias[:, par] + taps[2:3, par] * gate + taps[1:2, par] * later(gate, 1)
                        + taps[0:1, par] * later(gate, 2))
                out = conv / (1.0 + jnp.exp(-conv)) * up
                if keep:
                    conv_s[seq, cols] = conv
                    up_s[seq, cols] = up
                    hid_t[at(j * tile, tile), seq] = out.T.astype(jnp.bfloat16)
                else:
                    hid[seq, cols] = out.astype(jnp.bfloat16)

    def to_owners(o, into, send_sems, recv_sems, act):
        for d, peer in enumerate((qa, qb, qd)):
            src = gp.at[:, at(o * wide + peer * r, r)]
            act(remote(src, into.at[at(q * u, u), :], send_sems.at[d], recv_sems.at[d], fs=base + peer))

    def keep_own(o, into):
        into[at(q * u, u), :] = gp[:, at(o * wide + q * r, r)]

    def exchange(act):
        to_owners(z, hand, g_s, g_r, act)

    def passing_r(act):
        to_owners(nz - 1, passed_r, pr_s, pr_r, act)

    def passing_l(act):
        to_owners(0, passed_l, pl_s, pl_r, act)

    def passed_on_r():
        return remote(passed_r, passed_r, fr_s.at[0], fr_r.at[0], fs=f + GROUP)

    def passed_on_l():
        return remote(passed_l, passed_l, fl_s.at[0], fl_r.at[0], fs=f - GROUP)

    arrival = lambda copy: copy.wait_recv()

    def hand_on():
        @pl.when(z == nz - 2)
        def _():
            passing_r(arrival)
            passed_on_r().start()

        @pl.when(z == 1)
        def _():
            passing_l(arrival)
            passed_on_l().start()

    def slot_r(o, m, e):
        there = gin_r.at[m, :, pl.ds(e * part, part)]
        return remote(gp.at[:, at(o * wide + e * part, part)], there, zr_s.at[m, e], zr_r.at[m, e], fs=f + GROUP)

    def slot_l(o, m, e):
        there = gin_l.at[m, :, pl.ds(e * part, part)]
        return remote(gp.at[:, at(o * wide + e * part, part)], there, zl_s.at[m, e], zl_r.at[m, e], fs=f - GROUP)

    halves = range(parts_d)

    def pass_part(o, into, send_sems, recv_sems, e):
        for d, peer in enumerate((qa, qb, qd)):
            @pl.when(lax.div(peer * r, part) == e)
            def _(d=d, peer=peer):
                src = gp.at[:, at(o * wide + peer * r, r)]
                remote(src, into.at[at(q * u, u), :], send_sems.at[d], recv_sems.at[d], fs=base + peer).start()
        if e == parts_d - 1:
            keep_own(o, into)

    def rightward(o, m, e):
        if m < nz - 2:
            slot_r(o, m, e).start()
            return

        @pl.when(z == nz - 2)
        def _():
            pass_part(nz - 1, passed_r, pr_s, pr_r, e)

        @pl.when(z < nz - 2)
        def _():
            slot_r(o, m, e).start()

    def leftward(o, m, e):
        if m < nz - 2:
            slot_l(o, m, e).start()
            return

        @pl.when(z == 1)
        def _():
            pass_part(0, passed_l, pl_s, pl_r, e)

        @pl.when(z > 1)
        def _():
            slot_l(o, m, e).start()

    def down_grad():
        for i in range(nz):
            o = nz - 1 - i + upper * (2 * i - (nz - 1))
            cols = at(o * wide, wide)
            cot = t2[:, :, cols].reshape(GROUP * rows, wide)
            gp[:, cols] = mm(hid_t[...], cot).astype(jnp.bfloat16)
            if i < nz - 1:
                @pl.when(low)
                def _():
                    for e in halves:
                        rightward(o, i, e)

                @pl.when(high)
                def _():
                    for e in halves:
                        leftward(o, i, e)

        @pl.when(jnp.logical_or(low, high))
        def _():
            exchange(begin)

    def settle():
        @pl.when(jnp.logical_and(first, last))
        def _():
            m = nz - 2
            for e in halves:
                slot_r(z, m, e).wait_recv()
                slot_l(z, m, e).wait_recv()
            home = gp.at[:, at(z * wide, wide)]
            total(home, [home, gin_r.at[m], gin_l.at[m]], u)
            exchange(begin)

    def chain(j, e):
        o, p = nz - 2 + z - j, z + 2 - nz + j
        here = pl.ds(e * part, part)

        @pl.when(jnp.logical_and(first, o <= nz - 1))
        def _():
            slot_r(o, j, e).wait_recv()
            cols = at(o * wide + e * part, part)
            total(gp.at[:, cols], [gp.at[:, cols], gin_r.at[j, :, here]], u)
            rightward(o, j + 1, e)

        @pl.when(jnp.logical_and(last, p >= 0))
        def _():
            slot_l(p, j, e).wait_recv()
            cols = at(p * wide + e * part, part)
            total(gp.at[:, cols], [gp.at[:, cols], gin_l.at[j, :, here]], u)
            leftward(p, j + 1, e)

    def backward(n):
        b, out = order[n], pl.ds(n * rows, rows)

        @pl.loop(0, u // tile)
        def _(j):
            cols, seq, par = at(j * tile, tile), at(b * rows, rows), at(units + j * tile, tile)
            dh = mm(t2[b], od[at(j * tile, tile), :], ((1,), (1,)))
            conv = conv_s[seq, cols]
            sig = 1.0 / (1.0 + jnp.exp(-conv))
            dup[out, cols] = (dh * (conv * sig)).astype(jnp.bfloat16)
            dc = dh * up_s[seq, cols] * sig * (1.0 + conv * (1.0 - sig))
            dg = (taps[2:3, par] * dc + taps[1:2, par] * earlier(dc, 1)
                  + taps[0:1, par] * earlier(dc, 2))
            dgate[out, cols] = dg.astype(jnp.bfloat16)

    mirrored = z + upper * (nz - 1 - 2 * z)

    def turn(i):
        near_side = lax.div(mirrored - i + nz, nz)
        v = i + near_side * (mirrored - 2 * i)
        return v + upper * (nz - 1 - 2 * v)


    def late_start(h):
        return turn(h // parts_d) * wide + h % parts_d * part if isinstance(h, int) else (
            turn(lax.div(h, parts_d)) * wide + lax.rem(h, parts_d) * part)

    def late_block(h):
        cols = at(late_start(h), part)
        yp[:, cols] = mm(hid[...], od[:, cols]).astype(jnp.bfloat16)

    parts, finals, results = (yp, xp), (y, dx), (y_out, dx_out)
    order = (qd, qa, qb, q)
    theirs = (qd, qb, qa, q)
    places = ((order, theirs), ((0, 1, 2, 3), (0, 2, 1, 3)))

    def span(t, i):
        return at(late_start(i), part) if t == 0 else at(i * wide, wide)

    def core_copy(t, i, n):
        cols = span(t, i)
        src = parts[t].at[at(places[t][1][n] * rows + (1 - c) * half, half), cols]
        return remote(src, core.at[t, n, :, cols], c_s.at[t, i, n], c_r.at[t, i, n], tp=1 - c)

    def to_core(t, i):
        for n in range(4):
            core_copy(t, i, n).start()

    def plane_copy(t, i, slot):
        cols = span(t, i)
        src = core.at[t, 0, :, cols] if slot == 2 else summed.at[t, slot, :, cols]
        return remote(src, got.at[t, slot, :, cols], a_s.at[t, i, slot], a_r.at[t, i, slot],
                      fs=base + (qb if slot == 2 else qa))

    def join_one(t, i, n):
        cols = span(t, i)
        core_copy(t, i, n).wait_recv()
        own = parts[t].at[at(places[t][0][n] * rows + c * half, half), cols]
        total(summed.at[t, n, :, cols], [own, core.at[t, n, :, cols]], half)
        if n < 2:
            plane_copy(t, i, n).start()

    def join(t, i):
        for n in range(4):
            join_one(t, i, n)

    def second(t, i):
        cols = span(t, i)
        plane_copy(t, i, 0).wait_recv()
        total(core.at[t, 0, :, cols], [summed.at[t, 2, :, cols], got.at[t, 0, :, cols]], half)
        plane_copy(t, i, 2).start()

    def end_copy(t, i):
        cols = span(t, i)
        return remote(finals[t].at[:, cols], results[t].at[mine, cols], e_s.at[t, i], e_r.at[t, i], tp=1 - c)

    def own_copy(t, i):
        cols = span(t, i)
        return pltpu.make_async_copy(finals[t].at[:, cols], results[t].at[mine, cols], o_s.at[t, i])

    def finish(t, i):
        cols = span(t, i)
        plane_copy(t, i, 1).wait_recv()
        plane_copy(t, i, 2).wait_recv()
        total(finals[t].at[:, cols], [summed.at[t, 3, :, cols], got.at[t, 1, :, cols], got.at[t, 2, :, cols]], half)
        end_copy(t, i).start()
        own_copy(t, i).start()

    blocks = (nz * parts_d, nz)

    def each(fn, t=1):
        @pl.loop(0, blocks[t])
        def _(i):
            fn(i)

    def early_piece(n, m, i):
        seq, cols = pl.ds(n * rows, m * rows), at(i * wide, wide)
        out = mm(dup[seq, :], ou[cols, :], ((1,), (1,))) + mm(dgate[seq, :], og[cols, :], ((1,), (1,)))
        xp[seq, cols] = out.astype(jnp.bfloat16)
        for k in range(n, n + m):
            core_copy(1, i, (0, 2, 1, 3)[k]).start()

    def first_out():
        for i in range(nz + 2):
            if i < nz:
                early_piece(0, 1, i)
            if i > 1:
                join_one(1, i - 2, 0)

    def pair_out():
        for i in range(nz + 1):
            if i < nz:
                early_piece(1, 2, i)
            if i > 0:
                join_one(1, i - 1, 2)
                join_one(1, i - 1, 1)
            if 1 < i < nz:
                second(1, i - 2)

    def last_out():
        each(lambda i: early_piece(3, 1, i))

    def joins(n):
        each(lambda i: join_one(1, i, n))

    def finishes(t):
        each(lambda i: finish(t, i), t)

    def ended_out(t):
        each(lambda i: end_copy(t, i).wait_recv(), t)

    partner, far = [], {}

    def pass_on(i, owner, kind):
        there = ts[i].at[owner, mine, :]
        copy = remote(there, there, p_s.at[i, kind], p_r.at[i, kind], tp=1 - c)
        copy.start()
        partner.append(copy)

    def adjacent(i):
        near[i, 0].wait_recv()
        there = ts[i].at[qa, mine, :]
        copy = remote(there, there, n_s.at[i, 2], n_r.at[i, 2], fs=base + qb)
        copy.start()
        far[i] = copy
        pass_on(i, qa, 0)
        near[i, 1].wait_recv()
        pass_on(i, qb, 1)

    def opposite(i):
        far[i].wait_recv()
        pass_on(i, qd, 2)

    def complete(i):
        for kind, owner in enumerate((qb, qa, qd)):
            there = ts[i].at[owner, other, :]
            remote(there, there, p_s.at[i, kind], p_r.at[i, kind], tp=1 - c).wait_recv()
        local[3 + i].wait()

    for k in range(2):
        for d, peer in enumerate((qa, qb, qd)):
            weights[k, d].wait_recv()
            along(k, landing(k, base + peer), base + peer)
        local[k].wait()
    adjacent(1)
    if nz > 2:
        relay(0, 0)
        relay(1, 0)
    adjacent(0)
    for d in range(3):
        weights[2, d].wait_recv()
    local[2].wait()
    for s in range(1, nz - 2):
        relay(0, s)
        relay(1, s)
    for k in downs:
        onward(k, 0, begin)
    adjacent(2)
    at_end = jnp.logical_or(low, high) if nz > 1 else z < 0
    inside = jnp.logical_and(first, last) if nz > 1 else z >= 0

    def forward_head(i):
        @pl.when(at_end)
        def _():
            begun(i)

        @pl.when(inside)
        def _():
            forward(i, False)

    def forward_tail(i):
        @pl.when(at_end)
        def _():
            forward(i, True)

    opposite(1)
    complete(1)
    for s in range(nz - 2):
        ended(0, s)
        ended(1, s)
    if nz > 2:
        for k in downs:
            relay(k, 0)
    forward_head(1)
    opposite(0)
    complete(0)
    forward_head(0)
    for s in range(1, nz - 2):
        for k in downs:
            relay(k, s)
    if nz > 1:
        ended(0, nz - 2)
        ended(1, nz - 2)
    forward_tail(1)
    opposite(2)
    complete(2)
    down_grad()
    forward_tail(0)

    count = blocks[0]

    @pl.when(at_end)
    def _():
        progress = [0, 0]

        def catch_up(stage, upto):
            while progress[stage] <= upto:
                (join, second)[stage](0, progress[stage])
                progress[stage] += 1

        for h in range(count - 1):
            i, p = divmod(h, parts_d)
            if i > 0:
                ended(2 + p, i - 1)
            late_block(h)
            to_core(0, h)
            if h > 2:
                catch_up(1, h - 3)
            catch_up(0, h - 1)
            if h in (parts_d * (nz - 2) - 1, parts_d * (nz - 1) - 1):
                catch_up(0, h)
                catch_up(1, h - 1)
        catch_up(0, count - 2)
        catch_up(1, count - 3)
        if nz > 1:
            ended(1 + parts_d, nz - 2)
        late_block(count - 1)
        to_core(0, count - 1)

    @pl.when(inside)
    def _():
        for h in range(count):
            late_block(h)
            to_core(0, h)
            if h > 1:
                join(0, h - 2)
        for h in range(max(count - 2, 0), count - 1):
            join(0, h)

    def seconds_late(begin_at):
        @pl.loop(begin_at, count)
        def _(h):
            second(0, h)

    if nz > 2:
        chain(0, 0)
    def grad_sum(*extra):
        @pl.loop(0, GROUP * u, step=128)
        def _(i):
            sl = at(i, 128)
            out = hand[sl, :].astype(jnp.float32)
            for e in extra:
                out = out + e[sl, :].astype(jnp.float32)
            g[sl, :] = gd[sl, :] + out

    g_copy = pltpu.make_async_copy(g, g_out, loc.at[8])

    def grad_out():
        exchange(arrival)
        keep_own(z, hand)
        old_grad.wait()

        @pl.when(inside)
        def _():
            grad_sum()

        if nz > 1:
            @pl.when(high)
            def _():
                passed_on_r().wait_recv()
                grad_sum(passed_r)

            @pl.when(low)
            def _():
                passed_on_l().wait_recv()
                grad_sum(passed_l)

        g_copy.start()

    backward(0)
    join(0, count - 1)
    first_out()
    for e in range(1, parts_d if nz > 2 else 0):
        chain(0, e)

    @pl.when(at_end)
    def _():
        seconds_late(max(count - 2, 0))

    @pl.when(inside)
    def _():
        seconds_late(0)

    backward(1)
    backward(2)
    for j in range(1, nz - 2):
        for e in halves:
            chain(j, e)
    pair_out()
    if nz > 1:
        hand_on()
    for i in range(max(nz - 2, 0), nz):
        second(1, i)
    backward(3)
    if nz > 1:
        settle()
    last_out()
    joins(3)
    finishes(0)
    for copies in (weights, near, far):
        for copy in copies.values():
            copy.wait_send()
    for copy in partner:
        copy.wait_send()
    for s in range(nz - 1):
        for k in range(2 + parts_d):
            onward(k, s, sent)

    @pl.loop(0, count)
    def _(i):
        for n in range(4):
            core_copy(0, i, n).wait_send()
        for slot in range(3):
            plane_copy(0, i, slot).wait_send()

    for m in range(nz - 2):
        @pl.when(jnp.logical_and(last, z <= m))
        def _(m=m):
            for e in halves:
                slot_r(0, m, e).wait_send()

        @pl.when(jnp.logical_and(first, nz - 1 - z <= m))
        def _(m=m):
            for e in halves:
                slot_l(0, m, e).wait_send()

    if nz > 1:
        @pl.when(z < nz - 2)
        def _():
            for e in halves:
                slot_r(0, nz - 2, e).wait_send()

        @pl.when(z == nz - 2)
        def _():
            passing_r(sent)

        @pl.when(z > 1)
        def _():
            for e in halves:
                slot_l(0, nz - 2, e).wait_send()

        @pl.when(z == 1)
        def _():
            passing_l(sent)

    def settled():
        ended_out(0)

        @pl.loop(0, count)
        def _(i):
            end_copy(0, i).wait_send()
            own_copy(0, i).wait()

        @pl.loop(0, nz)
        def _(i):
            for n in range(4):
                core_copy(1, i, n).wait_send()
            for slot in range(2):
                plane_copy(1, i, slot).wait_send()

    @pl.when(at_end)
    def _():
        for i in range(nz - 1):
            finish(1, i)
        settled()
        grad_out()
        finish(1, nz - 1)

    @pl.when(inside)
    def _():
        finishes(1)
        settled()
        grad_out()

    ended_out(1)
    exchange(sent)

    @pl.loop(0, nz)
    def _(i):
        plane_copy(1, i, 2).wait_send()
        end_copy(1, i).wait_send()
        own_copy(1, i).wait()

    if nz > 1:
        @pl.when(z == nz - 2)
        def _():
            passed_on_r().wait_send()

        @pl.when(z == 1)
        def _():
            passed_on_l().wait_send()

    g_copy.wait()


def layer(nz, xs, w_gate, w_up, w_down, taps, bias, grad_down):
    rows, d = xs[0].shape
    u = w_gate.shape[1] // GROUP
    r = w_gate.shape[0]
    half, toks, wide = rows // 2, GROUP * rows, GROUP * r
    tile = 256 if u % 256 == 0 else 128
    sems = lambda *shape: [pltpu.SemaphoreType.DMA(shape)] * 2
    b16, f32 = jnp.bfloat16, jnp.float32
    out = jax.ShapeDtypeStruct((rows, d), b16)
    hops = max(nz - 1, 1)
    parts_d = wide // 256 if wide % 256 == 0 else 1
    count = nz * parts_d
    return pl.pallas_call(
        functools.partial(layer_kernel, nz, tile),
        out_shape=(out, out, jax.ShapeDtypeStruct((u * GROUP, r), f32)),
        in_specs=[ANY] * 6 + [VMEM] * 2 + [ANY],
        out_specs=(ANY,) * 3,
        scratch_shapes=[pltpu.VMEM((half, d), b16)] * 2
        + [pltpu.VMEM((u * GROUP, r), f32)] * 2
        + [pltpu.VMEM((GROUP, rows, d), b16)] * 3
        + [pltpu.VMEM((d, u), b16)] * 2
        + [pltpu.VMEM((u, d), b16), pltpu.VMEM((toks, u), b16), pltpu.VMEM((u, toks), b16),
           pltpu.VMEM((toks, u), f32), pltpu.VMEM((toks, u), f32),
           pltpu.VMEM((toks, u), f32), pltpu.VMEM((toks, u), f32),
           pltpu.VMEM((toks, u), b16), pltpu.VMEM((toks, u), b16),
           pltpu.VMEM((toks, d), b16), pltpu.VMEM((toks, d), b16), pltpu.VMEM((u, d), b16),
           pltpu.VMEM((2, 4, half, d), b16), pltpu.VMEM((2, 4, half, d), b16), pltpu.VMEM((2, 3, half, d), b16),
           pltpu.VMEM((hops, u, wide), b16), pltpu.VMEM((hops, u, wide), b16)]
        + [pltpu.VMEM((u * GROUP, r), b16)] * 3
        + [pltpu.SemaphoreType.DMA((10,))]
        + sems(3, 3) + sems(3, 3) + sems(3, 3) + sems(hops, 2 + parts_d) + sems(hops, 2 + parts_d)
        + sems(2, count, 4) + sems(2, count, 3) + sems(hops, parts_d) + sems(hops, parts_d) + sems(3)
        + sems(3) + sems(3) + sems(1) + sems(1) + sems(2, count)
        + [pltpu.SemaphoreType.DMA((2, count))],
        compiler_params=pltpu.CompilerParams(collective_id=0, has_side_effects=True, vmem_limit_bytes=VMEM_BYTES),
        name="layer_group",
    )(*xs, w_gate, w_up, w_down, taps, bias, grad_down)


def shift_later(field, steps):
    pad = jnp.zeros((steps, field.shape[1]), jnp.float32)
    return jnp.concatenate([pad, field[: field.shape[0] - steps]], axis=0)


def shift_earlier(field, steps):
    pad = jnp.zeros((steps, field.shape[1]), jnp.float32)
    return jnp.concatenate([field[steps:], pad], axis=0)


def contract_last(left, right):
    return lax.dot_general(
        left, right, (((1,), (1,)), ((), ())), preferred_element_type=jnp.float32
    )


def hidden_parts(inputs, gate_full, up_full, taps, bias):
    gate = (
        jnp.dot(inputs, gate_full, preferred_element_type=jnp.float32)
        .astype(jnp.bfloat16)
        .astype(jnp.float32)
    )
    up = jnp.dot(inputs, up_full, preferred_element_type=jnp.float32)
    conv = bias + taps[2] * gate + taps[1] * shift_later(gate, 1) + taps[0] * shift_later(gate, 2)
    act = jax.nn.silu(conv)
    hidden = (act * up).astype(jnp.bfloat16)
    return (conv, act, up, hidden)


def forward_pass(x_late, gate_full, up_full, down_full, taps, bias):
    conv, act, up, hidden = hidden_parts(x_late, gate_full, up_full, taps, bias)
    partial_value = jnp.dot(hidden, down_full, preferred_element_type=jnp.float32)
    return lax.psum(partial_value.astype(jnp.bfloat16), "tp")


def backward_pass(x_early, cotangent, gate_full, up_full, down_full, taps, bias, grad_down):
    conv, act, up, hidden = hidden_parts(x_early, gate_full, up_full, taps, bias)
    dhidden = contract_last(cotangent, down_full)
    summed = lax.psum_scatter(
        lax.dot_general(
            cotangent, hidden, (((0,), (0,)), ((), ())), preferred_element_type=jnp.float32
        ),
        "fs",
        scatter_dimension=0,
        tiled=True,
    )
    grad_down_out = grad_down + summed.T
    dup = (dhidden * act).astype(jnp.bfloat16)
    sig = jax.nn.sigmoid(conv)
    dconv = dhidden * up * sig * (1.0 + conv * (1.0 - sig))
    dgate = taps[2] * dconv + taps[1] * shift_earlier(dconv, 1) + taps[0] * shift_earlier(dconv, 2)
    dgate = dgate.astype(jnp.bfloat16)
    partial_value = contract_last(dup, up_full) + contract_last(dgate, gate_full)
    dx_early = lax.psum(partial_value.astype(jnp.bfloat16), "tp")
    return (dx_early, grad_down_out)


def shards(x_late, x_early, cotangent, w_gate, w_up, w_down, conv_taps, conv_bias, grad_down):
    width = w_gate.shape[1]
    offset = lax.axis_index("tp") * width
    taps = lax.dynamic_slice_in_dim(conv_taps, offset, width, 1)
    bias = lax.dynamic_slice_in_dim(conv_bias, offset, width, 0)
    gate_full, up_full = (
        lax.all_gather(w_gate, "fs", axis=0, tiled=True),
        lax.all_gather(w_up, "fs", axis=0, tiled=True),
    )
    down_full = lax.all_gather(w_down, "fs", axis=1, tiled=True)
    y_late = forward_pass(x_late, gate_full, up_full, down_full, taps, bias)
    dx_early, grad_down_out = backward_pass(
        x_early, cotangent, gate_full, up_full, down_full, taps, bias, grad_down
    )
    return (y_late, dx_early, grad_down_out)


def carry_kernel(pieces, *refs):
    ins, outs, held, r_s, w_s = refs[:3], refs[3:6], refs[6:9], refs[9], refs[10]

    def move(i, p, back):
        rows = ins[i].shape[0] // pieces
        sl = pl.ds(p * rows, rows)
        src, dst = (held[i], outs[i]) if back else (ins[i], held[i])
        return pltpu.make_async_copy(src.at[sl, :], dst.at[sl, :], (w_s if back else r_s).at[i, p])

    steps = [(i, p) for i in range(3) for p in range(pieces)]
    for i, p in steps:
        move(i, p, False).start()
    for i, p in steps:
        move(i, p, False).wait()
        move(i, p, True).start()
    for i, p in steps:
        move(i, p, True).wait()


def carry(*arrays):
    pieces = 2
    return pl.pallas_call(
        functools.partial(carry_kernel, pieces),
        out_shape=tuple(jax.ShapeDtypeStruct(a.shape, a.dtype) for a in arrays),
        in_specs=[ANY] * 3,
        out_specs=(ANY,) * 3,
        scratch_shapes=[pltpu.VMEM(a.shape, a.dtype) for a in arrays]
        + [pltpu.SemaphoreType.DMA((3, pieces))] * 2,
        compiler_params=pltpu.CompilerParams(vmem_limit_bytes=VMEM_BYTES),
        name="results",
    )(*arrays)


def grouped_shards(nz, x_late, x_early, cotangent, w_gate, w_up, w_down, conv_taps, conv_bias, grad_down):
    outputs = layer(
        nz, (x_late, x_early, cotangent), w_gate, w_up, w_down, conv_taps,
        conv_bias.reshape(1, conv_bias.shape[0]), grad_down,
    )
    return carry(*outputs)


def solution(mesh):
    def step(*arrays):
        x_late, w_gate = arrays[0], arrays[3]
        fs, tp = mesh.shape["fs"], mesh.shape["tp"]
        units, rest = divmod(w_gate.shape[1], GROUP)
        lanes_ok = rest == 0 and units % 128 == 0 and w_gate.shape[0] % 128 == 0
        if tp == 2 and fs % GROUP == 0 and lanes_ok and x_late.shape[0] % 32 == 0:
            return grouped_shards(fs // GROUP, *arrays)
        return shards(*arrays)

    placed = (
        P("fs", None),
        P("fs", None),
        P("fs", None),
        P("fs", "tp"),
        P("fs", "tp"),
        P("tp", "fs"),
        P(),
        P(),
        P("tp", "fs"),
    )
    return jax.shard_map(
        step,
        mesh=mesh,
        in_specs=placed,
        out_specs=(P("fs", None), P("fs", None), P("tp", "fs")),
        check_vma=False,
    )
```
